256 devices in a mesh: sp: 32 (over z, x), tp: 8 (over y, core).
Axes of the slice: x: 4, y: 4, z: 8, core: 2. Of those that a mesh axis runs over, the one named last changes fastest.
Arguments:
- features: bfloat16 [12288, 2048], P('sp', 'tp'), may hold values from -6 to 6
- norm_gain: float32 [2048], replicated, may hold values from 0.28 to 10
- w_query: bfloat16 [2048, 1024], P(None, 'tp'), may hold values from -0.125 to 0.125
- w_key: bfloat16 [2048, 512], P(None, 'tp'), may hold values from -0.125 to 0.125
- w_value: bfloat16 [2048, 512], P(None, 'tp'), may hold values from -0.125 to 0.125
- head_sinks: float32 [16], P('tp'), may hold values from 1 to 5
- w_query_latent: bfloat16 [2048, 512], replicated, may hold values from -0.125 to 0.125
- w_kv_latent: bfloat16 [2048, 512], replicated, may hold values from -0.125 to 0.125
- w_rope_key: bfloat16 [2048, 64], replicated, may hold values from -0.125 to 0.125
- query_latent_gain: float32 [512], replicated, may hold values from 0.28 to 10
- kv_latent_gain: float32 [512], replicated, may hold values from 0.28 to 10
- w_query_content: bfloat16 [512, 1024], P(None, 'tp'), may hold values from -0.25 to 0.25
- w_query_rotary: bfloat16 [512, 512], P(None, 'tp'), may hold values from -0.25 to 0.25
- w_key_up: bfloat16 [512, 1024], P(None, 'tp'), may hold values from -0.25 to 0.25
- w_value_up: bfloat16 [512, 1024], P(None, 'tp'), may hold values from -0.25 to 0.25
- w_branch_window: bfloat16 [1024, 2048], P('tp'), may hold values from -0.1875 to 0.1875
- w_branch_latent: bfloat16 [1024, 2048], P('tp'), may hold values from -0.1875 to 0.1875
- w_gate_window: bfloat16 [2048, 2048], P(None, 'tp'), may hold values from -0.125 to 0.125
- w_gate_latent: bfloat16 [2048, 2048], P(None, 'tp'), may hold values from -0.125 to 0.125
Outputs:
- mixed: bfloat16 [12288, 2048], P('sp', 'tp')
The draws below stay inside these ranges and needn't reach their ends.
All inputs are finite; a program needn't handle non-finite values.
Results may differ from the reference program's by a relative error of at most 0.018.
The reference program's roundings to bfloat16 on the way count: a program that leaves them out, or rounds other values in their place, can miss the bound.
Values may be sent and summed in bfloat16 or wider, within the bound.
A program may use at most 128 MiB of HBM per device.

```python
import jax
import jax.numpy as jnp
from jax import lax

D = 2048
Q_HEADS = 16
KV_HEADS = 8
HEAD = 64
WINDOW = 128
LAT_HEADS = 8
Q_LATENT = 512
KV_LATENT = 512
NOPE = 128
ROPE = 64
VDIM = 128
TOK_DEV = 384
SEQ = 12288


def gain_draw(key, length):
    return 1.0 + 0.18 * jnp.clip(jax.random.normal(key, (length,), jnp.float32), -4.0, 4.0)


def draw_norm_gain(key, part):
    return gain_draw(jax.random.fold_in(key, 11), D)


def draw_query_latent_gain(key, part):
    return gain_draw(jax.random.fold_in(key, 23), Q_LATENT)


def draw_kv_latent_gain(key, part):
    return gain_draw(jax.random.fold_in(key, 37), KV_LATENT)


def block_levels(stream_key, extent, cuts, smallest, top_value):
    def one(axis_at, blocks):
        steps = jax.random.uniform(jax.random.fold_in(jax.random.fold_in(stream_key, 6), axis_at), (blocks,), jnp.float32, smallest / len(cuts), top_value / len(cuts))
        return jnp.repeat(jnp.exp(steps), extent[axis_at] // blocks).reshape((-1,) + (1,) * (len(extent) - axis_at - 1))

    loudness = one(*cuts[0])
    for cut in cuts[1:]:
        loudness = loudness * one(*cut)
    return loudness


def normal_values(stream_key, dims, width, reach, pieces=(), kind=jnp.bfloat16):
    loudness = block_levels(stream_key, dims, pieces, -0.22, 0.18) if pieces else 1.0
    values = jax.random.normal(stream_key, dims, jnp.float32) * width * loudness
    return jnp.minimum(jnp.maximum(values, -reach), reach).astype(kind)


def setup_inputs(seed: int = 0) -> dict:
    key_of = jax.random.split(jax.random.key(seed), 20)
    return {
        "features": normal_values(key_of[0], (SEQ, D), 1.0, 6.0, ((0, 32), (1, 8))),
        "norm_gain": draw_norm_gain(jax.random.fold_in(key_of[19], 71), 0),
        "w_query": normal_values(key_of[2], (D, Q_HEADS * HEAD), D ** -0.5, 0.125, ((1, 8),)),
        "w_key": normal_values(key_of[3], (D, KV_HEADS * HEAD), D ** -0.5, 0.125, ((1, 8),)),
        "w_value": normal_values(key_of[4], (D, KV_HEADS * HEAD), D ** -0.5, 0.125, ((1, 8),)),
        "head_sinks": jnp.clip(1.0 + 4.0 * jax.random.uniform(key_of[5], (Q_HEADS,), jnp.float32) ** block_levels(key_of[5], (Q_HEADS,), ((0, 8),), -0.2, 0.2), 1.0, 5.0),
        "w_query_latent": normal_values(key_of[6], (D, Q_LATENT), D ** -0.5, 0.125),
        "w_kv_latent": normal_values(key_of[7], (D, KV_LATENT), D ** -0.5, 0.125),
        "w_rope_key": normal_values(key_of[8], (D, ROPE), D ** -0.5, 0.125),
        "query_latent_gain": draw_query_latent_gain(jax.random.fold_in(key_of[19], 71), 0),
        "kv_latent_gain": draw_kv_latent_gain(jax.random.fold_in(key_of[19], 71), 0),
        "w_query_content": normal_values(key_of[11], (Q_LATENT, LAT_HEADS * NOPE), Q_LATENT ** -0.5, 0.25, ((1, 8),)),
        "w_query_rotary": normal_values(key_of[12], (Q_LATENT, LAT_HEADS * ROPE), Q_LATENT ** -0.5, 0.25, ((1, 8),)),
        "w_key_up": normal_values(key_of[13], (KV_LATENT, LAT_HEADS * NOPE), KV_LATENT ** -0.5, 0.25, ((1, 8),)),
        "w_value_up": normal_values(key_of[14], (KV_LATENT, LAT_HEADS * VDIM), KV_LATENT ** -0.5, 0.25, ((1, 8),)),
        "w_branch_window": normal_values(key_of[15], (Q_HEADS * HEAD, D), (Q_HEADS * HEAD) ** -0.5, 0.1875, ((0, 8),)),
        "w_branch_latent": normal_values(key_of[16], (LAT_HEADS * VDIM, D), (LAT_HEADS * VDIM) ** -0.5, 0.1875, ((0, 8),)),
        "w_gate_window": normal_values(key_of[17], (D, D), D ** -0.5, 0.125, ((1, 8),)),
        "w_gate_latent": normal_values(key_of[18], (D, D), D ** -0.5, 0.125, ((1, 8),)),
    }


EPS = 1e-06
THETA = 10000.0
NEGATIVE = -1e+30

def rms_rows(float_rows, gain_vec):
    return float_rows * lax.rsqrt(lax.optimization_barrier(jnp.mean(float_rows * float_rows, axis=-1, keepdims=True)) + EPS) * gain_vec

def rotate(float_rows, positions):
    half_width = float_rows.shape[-1] // 2
    frequencies = THETA ** (-jnp.arange(half_width, dtype=jnp.float32) / half_width)
    angles = positions.astype(jnp.float32)[:, None] * frequencies
    target = (float_rows.shape[0],) + (1,) * (float_rows.ndim - 2) + (half_width,)
    cosine = jnp.cos(angles).reshape(target)
    sine_part = jnp.sin(angles).reshape(target)
    first_half = float_rows[..., :half_width]
    second_half = float_rows[..., half_width:]
    return jnp.concatenate([first_half * cosine - second_half * sine_part, second_half * cosine + first_half * sine_part], axis=-1)

def window_attention(queries, key_ext, value_ext, sink_table, row_start):
    row_count = queries.shape[0]
    kv_heads = key_ext.shape[1] // HEAD
    group_size = queries.shape[1] // HEAD // kv_heads
    blocks = row_count // WINDOW
    query_blocks = queries.reshape(blocks, WINDOW, kv_heads, group_size, HEAD).astype(jnp.float32)

    def banded(table):
        table = table.reshape(blocks + 1, WINDOW, kv_heads, HEAD)
        return jnp.concatenate([table[:-1], table[1:]], axis=1).astype(jnp.float32)
    key_band = banded(key_ext)
    value_band = banded(value_ext)
    scores = jnp.einsum('nqhgd,nkhd->nhgqk', query_blocks, key_band) * HEAD ** (-0.5)
    query_index = jnp.arange(WINDOW, dtype=jnp.int32)[:, None]
    key_index = jnp.arange(2 * WINDOW, dtype=jnp.int32)[None, :]
    offset = query_index + WINDOW - key_index
    key_position = row_start + jnp.arange(blocks, dtype=jnp.int32)[:, None, None] * WINDOW + key_index - WINDOW
    valid_mask = ((offset >= 0) & (offset < WINDOW) & (key_position >= 0))[:, None, None]
    scores = jnp.where(valid_mask, scores, NEGATIVE)
    sink_logit = sink_table.reshape(1, kv_heads, group_size, 1, 1)
    row_top = jnp.maximum(lax.optimization_barrier(jnp.max(scores, axis=-1, keepdims=True)), sink_logit)
    weights = jnp.where(valid_mask, jnp.exp(scores - row_top), 0.0)
    denominator = lax.optimization_barrier(jnp.sum(weights, axis=-1, keepdims=True)) + jnp.exp(sink_logit - row_top)
    probabilities = (weights / denominator).astype(jnp.bfloat16).astype(jnp.float32)
    attended = jnp.einsum('nhgqk,nkhd->nqhgd', probabilities, value_band)
    return attended.astype(jnp.bfloat16).reshape(row_count, kv_heads * group_size * HEAD)

def latent_attention(query_content, query_rotary, head_keys, head_values, rope_key):
    seq_rows = query_content.shape[0]
    lat_heads = query_content.shape[1]
    blocks = seq_rows // TOK_DEV
    scale_factor = (NOPE + ROPE) ** (-0.5)
    key_float = head_keys.astype(jnp.float32)
    value_float = head_values.astype(jnp.float32)
    rope_float = rope_key.astype(jnp.float32)
    content_blocks = query_content.reshape(blocks, TOK_DEV, lat_heads, NOPE)
    rotary_blocks = query_rotary.reshape(blocks, TOK_DEV, lat_heads, ROPE)
    key_position = jnp.arange(seq_rows, dtype=jnp.int32)

    def one_block(inputs):
        content_part, rotary_part, block_index = inputs
        scores = (jnp.einsum('qhd,khd->hqk', content_part.astype(jnp.float32), key_float) + jnp.einsum('qhr,kr->hqk', rotary_part.astype(jnp.float32), rope_float)) * scale_factor
        query_position = block_index * TOK_DEV + jnp.arange(TOK_DEV, dtype=jnp.int32)
        live_mask = key_position[None, :] <= query_position[:, None]
        scores = jnp.where(live_mask, scores, NEGATIVE)
        row_top = lax.optimization_barrier(jnp.max(scores, axis=-1, keepdims=True))
        weights = jnp.where(live_mask, jnp.exp(scores - row_top), 0.0)
        rounded = weights.astype(jnp.bfloat16).astype(jnp.float32)
        attended = jnp.einsum('hqk,khd->qhd', rounded, value_float)
        denominator = jnp.transpose(lax.optimization_barrier(jnp.sum(weights, axis=-1)))[:, :, None]
        return (attended / denominator).astype(jnp.bfloat16)
    result = lax.map(one_block, (content_blocks, rotary_blocks, jnp.arange(blocks, dtype=jnp.int32)))
    return result.reshape(seq_rows, lat_heads * VDIM)

def project(left, right):
    return jnp.dot(left, right, preferred_element_type=jnp.float32)

def reference(features, norm_gain, w_query, w_key, w_value, head_sinks, w_query_latent, w_kv_latent, w_rope_key, query_latent_gain, kv_latent_gain, w_query_content, w_query_rotary, w_key_up, w_value_up, w_branch_window, w_branch_latent, w_gate_window, w_gate_latent):
    seq_rows = features.shape[0]
    positions = jnp.arange(seq_rows, dtype=jnp.int32)
    normed = rms_rows(features.astype(jnp.float32), norm_gain).astype(jnp.bfloat16)
    query_rows = project(normed, w_query).astype(jnp.bfloat16)
    key_rows = project(normed, w_key).astype(jnp.bfloat16)
    value_rows = project(normed, w_value).astype(jnp.bfloat16)
    padding = jnp.zeros((WINDOW, key_rows.shape[1]), jnp.bfloat16)
    window_out = window_attention(query_rows, jnp.concatenate([padding, key_rows], axis=0), jnp.concatenate([padding, value_rows], axis=0), head_sinks, 0)
    latent_query = rms_rows(project(normed, w_query_latent), query_latent_gain).astype(jnp.bfloat16)
    latent_kv = rms_rows(project(normed, w_kv_latent), kv_latent_gain).astype(jnp.bfloat16)
    rope_key = rotate(project(normed, w_rope_key), positions).astype(jnp.bfloat16)
    query_content = project(latent_query, w_query_content).astype(jnp.bfloat16).reshape(seq_rows, LAT_HEADS, NOPE)
    query_rotary = rotate(project(latent_query, w_query_rotary).reshape(seq_rows, LAT_HEADS, ROPE), positions).astype(jnp.bfloat16)
    head_keys = project(latent_kv, w_key_up).astype(jnp.bfloat16).reshape(seq_rows, LAT_HEADS, NOPE)
    head_values = project(latent_kv, w_value_up).astype(jnp.bfloat16).reshape(seq_rows, LAT_HEADS, VDIM)
    latent_out = latent_attention(query_content, query_rotary, head_keys, head_values, rope_key)
    window_branch = project(window_out, w_branch_window)
    latent_branch = project(latent_out, w_branch_latent)
    window_gate = jax.nn.sigmoid(project(normed, w_gate_window))
    latent_gate = jax.nn.sigmoid(project(normed, w_gate_latent))
    return (window_gate * window_branch + latent_gate * latent_branch).astype(jnp.bfloat16)
```

```python
import functools
import math

import jax
import jax.numpy as jnp
from jax import lax
from jax.experimental import pallas as pl
from jax.experimental.pallas import tpu as pltpu
from jax.sharding import PartitionSpec as P

D = 2048
HEAD = 64
WINDOW = 128
NOPE = 128
ROPE = 64
VDIM = 128
LATENT = 512
ROWS = 384
COLS = 256
NX = 4
NY = 4
NZ = 8
NTP = 8
NSP = 32
EPS = 1e-06
THETA = 10000.0
NEGATIVE = -1e30
SOFT = (NOPE + ROPE) ** (-0.5) * math.log2(math.e)
MESH = pl.DeviceIdType.MESH
F32 = jnp.float32
BF16 = jnp.bfloat16


def dot(a, b):
    return jnp.dot(a, b, preferred_element_type=F32)


def contract(a, b, da, db):
    return lax.dot_general(a, b, (((da,), (db,)), ((), ())), preferred_element_type=F32)


def layer(
    x_ref, gain_ref, table_ref, qgain_ref, kvgain_ref, sink_ref,
    wq_h, wk_h, wv_h, wql_h, wkvl_h, wr_h, wqc_h, wqr_h, wku_h, wvu_h, wbw_h, wbl_h, wgw_h, wgl_h,
    out_ref,
    feats, normed,
    wq, wk, wv, wql, wkvl, wr, wqc, wqr, wku, wvu, wgw, wgl,
    colw, coll, kbuf, rvbuf, qbuf, ext, qwin, gatew, gatel,
    m_s, l_s, acc, o_send, st_send, o_recv, st_recv, wout, lat,
    w_sem, fs_sem, fr_sem, ks_sem, kr_sem, vs_sem, vr_sem, qs_sem, qr_sem, ts_sem, tr_sem,
    bs_sem, br_sem, os_sem, or_sem, ss_sem, sr_sem, ws_sem, wr_sem, ls_sem, lr_sem,
):
    sp = lax.axis_index("sp")
    tp = lax.axis_index("tp")
    z = sp // NX
    x = sp % NX
    y = tp // 2
    c = tp % 2

    def z_peer(by):
        return (((z + by + NZ) % NZ) * NX + x, tp)

    def x_peer(by):
        return (z * NX + (x + by + NX) % NX, tp)

    def y_peer(by):
        return (sp, ((y + by + NY) % NY) * 2 + c)

    def tp_peer(by):
        return (sp, (tp + by + NTP) % NTP)

    def sp_peer(by):
        return ((sp + by + NSP) % NSP, tp)

    sibling = (sp, tp + 1 - 2 * c)

    def remote(src, dst, ssem, rsem, dev):
        return pltpu.make_async_remote_copy(
            src_ref=src, dst_ref=dst, send_sem=ssem, recv_sem=rsem, device_id=dev, device_id_type=MESH
        )

    own_cols = pl.ds(pl.multiple_of(tp * COLS, COLS), COLS)
    pairs = [
        (wkvl_h, wkvl), (wr_h, wr), (wku_h, wku), (wvu_h, wvu), (wql_h, wql), (wqc_h, wqc), (wqr_h, wqr),
        (wq_h, wq), (wk_h, wk), (wv_h, wv), (wgw_h, wgw), (wgl_h, wgl),
        (wbw_h.at[:, own_cols], colw.at[0]), (wbl_h.at[:, own_cols], coll.at[0]),
        (x_ref, feats.at[0]),
    ]
    loads = [pltpu.make_async_copy(a, b, w_sem.at[i]) for i, (a, b) in enumerate(pairs)]
    (L_KVL, L_R, L_KU, L_VU, L_QL, L_QC, L_QR, L_Q, L_K, L_V, L_GW, L_GL, L_BW, L_BL, L_X) = range(15)
    loads[L_X].start()
    for i in range(14):
        loads[i].start()

    barrier = pltpu.get_barrier_semaphore()
    partners = [z_peer(1), z_peer(-1), sp_peer(1), sp_peer(-1)]
    partners += [x_peer(d) for d in range(1, NX)]
    partners += [tp_peer(d) for d in range(1, NTP)]
    for dev in partners:
        pl.semaphore_signal(barrier, inc=1, device_id=dev, device_id_type=MESH)
    pl.semaphore_wait(barrier, len(partners))
    loads[L_X].wait()

    half = ROWS // 2
    top, bot = pl.ds(0, half), pl.ds(half, half)

    def feat(i, src, dst, dev):
        return remote(src, dst, fs_sem.at[i], fr_sem.at[i], dev)

    f_sib = feat(0, feats.at[0], feats.at[1], sibling)
    f_rt = feat(1, feats.at[0, top], feats.at[2, top], y_peer(1))
    f_rb = feat(2, feats.at[0, bot], feats.at[2, bot], y_peer(1))
    f_lb = feat(3, feats.at[0, bot], feats.at[6, bot], y_peer(-1))
    f_lt = feat(4, feats.at[0, top], feats.at[6, top], y_peer(-1))
    f_ft = feat(5, feats.at[2, top], feats.at[4, top], y_peer(1))
    f_fb = feat(6, feats.at[6, bot], feats.at[4, bot], y_peer(-1))
    h_lt = feat(7, feats.at[2, top], feats.at[3, top], sibling)
    h_lb = feat(8, feats.at[2, bot], feats.at[3, bot], sibling)
    h_rb = feat(9, feats.at[6, bot], feats.at[7, bot], sibling)
    h_rt = feat(10, feats.at[6, top], feats.at[7, top], sibling)
    h_ft = feat(11, feats.at[4, top], feats.at[5, top], sibling)
    h_fb = feat(12, feats.at[4, bot], feats.at[5, bot], sibling)
    for cp in (f_rt, f_lb, f_rb, f_lt, f_sib):
        cp.start()
    f_rt.wait_recv()
    f_ft.start()
    h_lt.start()
    f_lb.wait_recv()
    f_fb.start()
    h_rb.start()
    f_rb.wait_recv()
    h_lb.start()
    f_lt.wait_recv()
    h_rt.start()

    def squares(i):
        v = feats[i].astype(F32)
        v = v * v
        return v[:, :128] + v[:, 128:]

    f_sib.wait_recv()
    total = squares(0) + squares(1) + squares(2) + squares(6)
    h_lt.wait_recv()
    h_lb.wait_recv()
    h_rb.wait_recv()
    h_rt.wait_recv()
    total = total + squares(3) + squares(7)
    f_ft.wait_recv()
    h_ft.start()
    f_fb.wait_recv()
    h_fb.start()
    total = total + squares(4)
    h_ft.wait_recv()
    h_fb.wait_recv()
    total = total + squares(5)
    inv = lax.rsqrt(jnp.sum(total, axis=-1, keepdims=True) * (1.0 / D) + EPS)

    branch = []
    for d in range(1, NTP):
        peer = (tp + d) % NTP
        cols = pl.ds(pl.multiple_of(peer * COLS, COLS), COLS)
        branch.append(remote(wbw_h.at[:, cols], colw.at[d], bs_sem.at[d - 1], br_sem.at[d - 1], (sp, peer)))
        branch.append(remote(wbl_h.at[:, cols], coll.at[d], bs_sem.at[d + 6], br_sem.at[d + 6], (sp, peer)))
    for cp in branch:
        cp.start()

    for i in range(8):
        dy, dc = i // 2, i % 2
        src = ((y - dy + NY) % NY) * 2 + (c if dc == 0 else 1 - c)
        cols = pl.ds(pl.multiple_of(src * COLS, COLS), COLS)
        normed[:, cols] = (feats[i].astype(F32) * inv * gain_ref[:, cols]).astype(BF16)

    def rms(v, g):
        return (v * lax.rsqrt(jnp.mean(v * v, axis=-1, keepdims=True) + EPS) * g[...]).astype(BF16)

    cos_t = table_ref[0:32, :]
    sin_t = table_ref[32:64, :]

    def rotate_t(v):
        a, b = v[:32], v[32:]
        return jnp.concatenate([a * cos_t - b * sin_t, b * cos_t + a * sin_t], axis=0)

    loads[L_KVL].wait()
    loads[L_R].wait()
    loads[L_KU].wait()
    loads[L_VU].wait()
    lkv = rms(dot(normed[...], wkvl[...]), kvgain_ref)
    kbuf[0] = dot(lkv, wku[...]).astype(BF16)
    rvbuf[0, 64:192] = jnp.transpose(dot(lkv, wvu[...])).astype(BF16)
    rvbuf[0, 0:64] = rotate_t(jnp.transpose(dot(normed[...], wr[...]))).astype(BF16)

    def k_copy(i, src, dst, dev):
        return remote(kbuf.at[src], kbuf.at[dst], ks_sem.at[i], kr_sem.at[i], dev)

    def v_copy(i, src, dst, dev):
        return remote(rvbuf.at[src], rvbuf.at[dst], vs_sem.at[i], vr_sem.at[i], dev)

    up, down = z_peer(1), z_peer(-1)
    ups = [(0, 0, 1), (1, 1, 2), (2, 2, 3)]
    downs = [(3, 0, 4), (4, 4, 5), (5, 5, 6)]
    k_up = [k_copy(*t, up) for t in ups]
    v_up = [v_copy(*t, up) for t in ups]
    k_dn = [k_copy(*t, down) for t in downs]
    v_dn = [v_copy(*t, down) for t in downs]
    k_far = k_copy(6, 6, 7, down)
    v_far = v_copy(6, 3, 7, up)
    k_up[0].start()
    k_dn[0].start()
    v_up[0].start()
    v_dn[0].start()

    loads[L_QL].wait()
    loads[L_QC].wait()
    loads[L_QR].wait()
    lq = rms(dot(normed[...], wql[...]), qgain_ref)
    qbuf[0, 0:128] = jnp.transpose(dot(lq, wqc[...])).astype(BF16)
    qbuf[0, 128:192] = rotate_t(jnp.transpose(dot(lq, wqr[...]))).astype(BF16)
    q_cp = [
        remote(qbuf.at[0], qbuf.at[d], qs_sem.at[d - 1], qr_sem.at[d - 1], x_peer(d)) for d in range(1, NX)
    ]
    for cp in q_cp:
        cp.start()

    loads[L_Q].wait()
    loads[L_K].wait()
    loads[L_V].wait()
    w3 = jnp.concatenate([wq[...], wk[...], wv[...]], axis=1)
    rows3 = dot(normed[...], w3).astype(BF16)
    qwin[...] = rows3[:, :128]
    ext[WINDOW:, :] = rows3[:, 128:]
    tail = remote(ext.at[pl.ds(ROWS, WINDOW)], ext.at[pl.ds(0, WINDOW)], ts_sem, tr_sem, sp_peer(1))
    tail.start()

    loads[L_GW].wait()
    loads[L_GL].wait()
    gatew[...] = jax.nn.sigmoid(dot(normed[...], wgw[...]))
    gatel[...] = jax.nn.sigmoid(dot(normed[...], wgl[...]))

    tail.wait_recv()
    ki = lax.broadcasted_iota(jnp.int32, (256, 256), 0)
    ci = lax.broadcasted_iota(jnp.int32, (256, 256), 1)
    offset = jnp.where(ci < 128, ci, ci - 128) + WINDOW - ki
    band = (offset >= 0) & (offset < WINDOW)
    first = lax.broadcasted_iota(jnp.int32, (1, 256), 1) < 128
    sink = jnp.where(first, sink_ref[0], sink_ref[1])
    for n in range(ROWS // WINDOW):
        lo = n * WINDOW
        q2 = jnp.concatenate([qwin[lo : lo + 128, 0:64], qwin[lo : lo + 128, 64:128]], axis=0)
        kv = ext[lo : lo + 256, :]
        s = contract(kv[:, 0:64], q2, 1, 1) * HEAD ** (-0.5)
        valid = band & (sp * ROWS + lo - WINDOW + ki >= 0)
        s = jnp.where(valid, s, NEGATIVE)
        peak = jnp.maximum(jnp.max(s, axis=0, keepdims=True), sink)
        w = jnp.where(valid, jnp.exp(s - peak), 0.0)
        den = jnp.sum(w, axis=0, keepdims=True) + jnp.exp(sink - peak)
        p = (w / den).astype(BF16)
        o = contract(p, kv[:, 64:128], 0, 0).astype(BF16)
        wout[0, lo : lo + 128, :] = jnp.concatenate([o[:128], o[128:]], axis=1)
    w_cp = [
        remote(wout.at[0], wout.at[d], ws_sem.at[d - 1], wr_sem.at[d - 1], tp_peer(d)) for d in range(1, NTP)
    ]
    for cp in w_cp:
        cp.start()

    m_s[...] = jnp.full((NX, 1, ROWS), NEGATIVE, F32)
    l_s[...] = jnp.zeros((NX, 1, ROWS), F32)
    acc[...] = jnp.zeros((NX, VDIM, ROWS), F32)

    def tile(keys, vals, d, masked):
        s = dot(keys, qbuf[d])
        if masked:
            kpos = lax.broadcasted_iota(jnp.int32, (ROWS, ROWS), 0)
            qpos = lax.broadcasted_iota(jnp.int32, (ROWS, ROWS), 1)
            s = jnp.where(kpos <= qpos, s, NEGATIVE)
        m_old = m_s[d]
        m_new = jnp.maximum(m_old, jnp.max(s, axis=0, keepdims=True))
        p = jnp.exp2((s - m_new) * SOFT)
        alpha = jnp.exp2((m_old - m_new) * SOFT)
        m_s[d] = m_new
        l_s[d] = l_s[d] * alpha + jnp.sum(p, axis=0, keepdims=True)
        acc[d] = acc[d] * alpha + dot(vals, p.astype(BF16))

    def block(slot):
        keys = jnp.concatenate([kbuf[slot], jnp.transpose(rvbuf[slot, 0:64])], axis=1)
        return keys, rvbuf[slot, 64:192]

    def whole(slot):
        keys, vals = block(slot)

        @pl.loop(0, NX)
        def _(d):
            tile(keys, vals, d, False)

    for cp in q_cp:
        cp.wait_recv()
    keys0, vals0 = block(0)
    tile(keys0, vals0, 0, True)

    @pl.loop(1, NX)
    def _(d):
        @pl.when(d > x)
        def _():
            tile(keys0, vals0, d, False)

    for k in range(1, 4):
        k_up[k - 1].wait_recv()
        if k < 3:
            k_up[k].start()
        k_dn[k - 1].wait_recv()
        if k < 3:
            k_dn[k].start()
        else:
            k_far.start()
        v_up[k - 1].wait_recv()
        if k < 3:
            v_up[k].start()
        else:
            v_far.start()
        v_dn[k - 1].wait_recv()
        if k < 3:
            v_dn[k].start()

        @pl.when(z >= k)
        def _():
            whole(k)

        @pl.when(z + k >= NZ)
        def _():
            whole(3 + k)

    k_far.wait_recv()
    v_far.wait_recv()

    @pl.when(z >= 4)
    def _():
        whole(7)

    o_cp = []
    for d in range(1, NX):
        o_send[d - 1] = acc[d].astype(BF16)
        st_send[d - 1, 0:1] = m_s[d]
        st_send[d - 1, 1:2] = l_s[d]
        o_cp.append(remote(o_send.at[d - 1], o_recv.at[d - 1], os_sem.at[d - 1], or_sem.at[d - 1], x_peer(-d)))
        o_cp.append(remote(st_send.at[d - 1], st_recv.at[d - 1], ss_sem.at[d - 1], sr_sem.at[d - 1], x_peer(-d)))
    for cp in o_cp:
        cp.start()

    for cp in branch:
        cp.wait_recv()
    loads[L_BW].wait()
    loads[L_BL].wait()
    for cp in w_cp:
        cp.wait_recv()
    allw = jnp.concatenate([wout[d] for d in range(NTP)], axis=1)
    gatew[...] = gatew[...] * dot(allw, colw[...].reshape(NTP * 128, COLS))

    for cp in o_cp:
        cp.wait_recv()
    ms = [m_s[0]] + [st_recv[d, 0:1] for d in range(3)]
    ls = [l_s[0]] + [st_recv[d, 1:2] for d in range(3)]
    top_m = jnp.maximum(jnp.maximum(ms[0], ms[1]), jnp.maximum(ms[2], ms[3]))
    ws = [jnp.exp2((m - top_m) * SOFT) for m in ms]
    den = ls[0] * ws[0] + ls[1] * ws[1] + ls[2] * ws[2] + ls[3] * ws[3]
    o = acc[0] * ws[0]
    for d in range(3):
        o = o + o_recv[d].astype(F32) * ws[d + 1]
    lat[0] = jnp.transpose(o / den).astype(BF16)
    l_cp = [
        remote(lat.at[0], lat.at[d], ls_sem.at[d - 1], lr_sem.at[d - 1], tp_peer(d)) for d in range(1, NTP)
    ]
    for cp in l_cp:
        cp.start()
    for cp in l_cp:
        cp.wait_recv()
    alll = jnp.concatenate([lat[d] for d in range(NTP)], axis=1)
    out_ref[...] = (gatew[...] + gatel[...] * dot(alll, coll[...].reshape(NTP * 128, COLS))).astype(BF16)

    sent = [f_sib, f_rt, f_rb, f_lb, f_lt, f_ft, f_fb, h_lt, h_lb, h_rb, h_rt, h_ft, h_fb]
    sent += branch + k_up + k_dn + v_up + v_dn + [k_far, v_far] + q_cp + [tail] + w_cp + o_cp + l_cp
    for cp in sent:
        cp.wait_send()


def on_device(
    features, norm_gain, w_query, w_key, w_value, head_sinks, w_query_latent, w_kv_latent, w_rope_key,
    query_latent_gain, kv_latent_gain, w_query_content, w_query_rotary, w_key_up, w_value_up,
    w_branch_window, w_branch_latent, w_gate_window, w_gate_latent,
):
    positions = lax.axis_index("sp") * ROWS + jnp.arange(ROWS, dtype=jnp.int32)
    frequencies = THETA ** (-jnp.arange(ROPE // 2, dtype=F32) / (ROPE // 2))
    angles = frequencies[:, None] * positions.astype(F32)[None, :]
    table = jnp.concatenate([jnp.cos(angles), jnp.sin(angles)], axis=0)
    vmem = pl.BlockSpec(memory_space=pltpu.VMEM)
    anyspace = pl.BlockSpec(memory_space=pl.ANY)
    smem = pl.BlockSpec(memory_space=pltpu.SMEM)
    dma = pltpu.SemaphoreType.DMA
    scratch = [
        pltpu.VMEM((8, ROWS, COLS), BF16),
        pltpu.VMEM((ROWS, D), BF16),
    ]
    weights = [
        w_query, w_key, w_value, w_query_latent, w_kv_latent, w_rope_key, w_query_content, w_query_rotary,
        w_key_up, w_value_up, w_branch_window, w_branch_latent, w_gate_window, w_gate_latent,
    ]
    scratch += [pltpu.VMEM(w.shape, BF16) for w in weights[:10] + weights[12:]]
    scratch += [
        pltpu.VMEM((NTP, 128, COLS), BF16),
        pltpu.VMEM((NTP, 128, COLS), BF16),
        pltpu.VMEM((8, ROWS, NOPE), BF16),
        pltpu.VMEM((8, ROPE + VDIM, ROWS), BF16),
        pltpu.VMEM((NX, NOPE + ROPE, ROWS), BF16),
        pltpu.VMEM((ROWS + WINDOW, 128), BF16),
        pltpu.VMEM((ROWS, 128), BF16),
        pltpu.VMEM((ROWS, COLS), F32),
        pltpu.VMEM((ROWS, COLS), F32),
        pltpu.VMEM((NX, 1, ROWS), F32),
        pltpu.VMEM((NX, 1, ROWS), F32),
        pltpu.VMEM((NX, VDIM, ROWS), F32),
        pltpu.VMEM((NX - 1, VDIM, ROWS), BF16),
        pltpu.VMEM((NX - 1, 2, ROWS), F32),
        pltpu.VMEM((NX - 1, VDIM, ROWS), BF16),
        pltpu.VMEM((NX - 1, 2, ROWS), F32),
        pltpu.VMEM((NTP, ROWS, 128), BF16),
        pltpu.VMEM((NTP, ROWS, 128), BF16),
    ]
    scratch += [
        dma((15,)), dma((13,)), dma((13,)), dma((7,)), dma((7,)), dma((7,)), dma((7,)),
        dma((3,)), dma((3,)), dma(()), dma(()), dma((14,)), dma((14,)),
        dma((3,)), dma((3,)), dma((3,)), dma((3,)), dma((7,)), dma((7,)), dma((7,)), dma((7,)),
    ]
    return pl.pallas_call(
        layer,
        out_shape=jax.ShapeDtypeStruct((ROWS, COLS), BF16),
        in_specs=[anyspace, vmem, vmem, vmem, vmem, smem] + [anyspace] * 14,
        out_specs=vmem,
        scratch_shapes=scratch,
        compiler_params=pltpu.CompilerParams(
            collective_id=0, has_side_effects=True, vmem_limit_bytes=60 * 1024 * 1024
        ),
    )(
        features, norm_gain.reshape(1, D), table, query_latent_gain.reshape(1, LATENT),
        kv_latent_gain.reshape(1, LATENT), head_sinks, *weights,
    )


def solution(mesh):
    return jax.shard_map(
        on_device,
        mesh=mesh,
        in_specs=(
            P("sp", "tp"), P(), P(None, "tp"), P(None, "tp"), P(None, "tp"), P("tp"), P(), P(), P(), P(), P(),
            P(None, "tp"), P(None, "tp"), P(None, "tp"), P(None, "tp"), P("tp", None), P("tp", None),
            P(None, "tp"), P(None, "tp"),
        ),
        out_specs=P("sp", "tp"),
        check_vma=False,
    )
```

```python
import functools
import math

import jax
import jax.numpy as jnp
from jax import lax
from jax.experimental import pallas as pl
from jax.experimental.pallas import tpu as pltpu
from jax.sharding import PartitionSpec as P

D = 2048
HEAD = 64
WINDOW = 128
NOPE = 128
ROPE = 64
VDIM = 128
LATENT = 512
ROWS = 384
COLS = 256
NX = 4
NY = 4
NZ = 8
NTP = 8
NSP = 32
EPS = 1e-06
THETA = 10000.0
NEGATIVE = -1e30
SOFT = (NOPE + ROPE) ** (-0.5) * math.log2(math.e)
MESH = pl.DeviceIdType.MESH
F32 = jnp.float32
BF16 = jnp.bfloat16


def dot(a, b):
    return jnp.dot(a, b, preferred_element_type=F32)


def contract(a, b, da, db):
    return lax.dot_general(a, b, (((da,), (db,)), ((), ())), preferred_element_type=F32)


def layer(
    x_ref, gain_ref, qgain_ref, kvgain_ref, sink_ref,
    wq_h, wkt_h, wvt_h, wql_h, wkvl_h, wrt_h, wqc_h, wqrt_h, wku_h, wvu_h, wbw_h, wbl_h, wgw_h, wgl_h,
    out_ref,
    feats, normed,
    wq, wrkv, wql, wkvl, wqc, wqrt, wku, wvu, wgw, wgl, trig,
    colw, coll, kbuf, rvbuf, qbuf, ext, qwin, gatew, gatel,
    m_s, l_s, acc, o_send, st_send, o_recv, st_recv, wout, lat,
    w_sem, fs_sem, fr_sem, ks_sem, kr_sem, vs_sem, vr_sem, qs_sem, qr_sem, ts_sem, tr_sem,
    bs_sem, br_sem, os_sem, or_sem, ss_sem, sr_sem, ws_sem, wr_sem, ls_sem, lr_sem,
):
    sp = lax.axis_index("sp")
    tp = lax.axis_index("tp")
    z = sp // NX
    x = sp % NX
    y = tp // 2
    c = tp % 2

    def z_peer(by):
        return (((z + by + NZ) % NZ) * NX + x, tp)

    def x_peer(by):
        return (z * NX + (x + by + NX) % NX, tp)

    def y_peer(by):
        return (sp, ((y + by + NY) % NY) * 2 + c)

    def tp_peer(by):
        return (sp, (tp + by + NTP) % NTP)

    def sp_peer(by):
        return ((sp + by + NSP) % NSP, tp)

    sibling = (sp, tp + 1 - 2 * c)

    def remote(src, dst, ssem, rsem, dev):
        return pltpu.make_async_remote_copy(
            src_ref=src, dst_ref=dst, send_sem=ssem, recv_sem=rsem, device_id=dev, device_id_type=MESH
        )

    own_cols = pl.ds(pl.multiple_of(tp * COLS, COLS), COLS)
    pairs = [
        (wkvl_h, wkvl), (wrt_h, wrkv.at[pl.ds(0, 64)]), (wku_h, wku), (wvu_h, wvu), (wql_h, wql), (wqc_h, wqc),
        (wqrt_h, wqrt), (wq_h, wq), (wkt_h, wrkv.at[pl.ds(64, 64)]), (wvt_h, wrkv.at[pl.ds(128, 64)]),
        (wgw_h, wgw), (wgl_h, wgl),
        (wbw_h.at[:, own_cols], colw.at[0]), (wbl_h.at[:, own_cols], coll.at[0]),
        (x_ref, feats.at[0]),
    ]
    loads = [pltpu.make_async_copy(a, b, w_sem.at[i]) for i, (a, b) in enumerate(pairs)]
    (L_KVL, L_R, L_KU, L_VU, L_QL, L_QC, L_QR, L_Q, L_K, L_V, L_GW, L_GL, L_BW, L_BL, L_X) = range(15)
    loads[L_X].start()
    for i in range(14):
        loads[i].start()

    barrier = pltpu.get_barrier_semaphore()
    partners = [z_peer(1), z_peer(-1), sp_peer(1), sp_peer(-1)]
    partners += [x_peer(d) for d in range(1, NX)]
    partners += [tp_peer(d) for d in range(1, NTP)]
    for dev in partners:
        pl.semaphore_signal(barrier, inc=1, device_id=dev, device_id_type=MESH)
    spots = lax.broadcasted_iota(jnp.int32, (ROPE // 2, ROWS), 1) + sp * ROWS
    freq_at = lax.broadcasted_iota(jnp.int32, (ROPE // 2, ROWS), 0)
    frequencies = jnp.exp(freq_at.astype(F32) * (-math.log(THETA) / (ROPE // 2)))
    angles = spots.astype(F32) * frequencies
    trig[0:32, :] = jnp.cos(angles)
    trig[32:64, :] = jnp.sin(angles)
    pl.semaphore_wait(barrier, len(partners))
    loads[L_X].wait()

    half = ROWS // 2
    top, bot = pl.ds(0, half), pl.ds(half, half)

    def spread(buf, ssem, rsem):
        def part(i, src, dst, rows, dev):
            return remote(buf.at[src, rows], buf.at[dst, rows], ssem.at[i], rsem.at[i], dev)

        return dict(
            sib=remote(buf.at[0], buf.at[1], ssem.at[0], rsem.at[0], sibling),
            rt=part(1, 0, 2, top, y_peer(1)),
            rb=part(2, 0, 2, bot, y_peer(1)),
            lb=part(3, 0, 6, bot, y_peer(-1)),
            lt=part(4, 0, 6, top, y_peer(-1)),
            ft=part(5, 2, 4, top, y_peer(1)),
            fb=part(6, 6, 4, bot, y_peer(-1)),
            hlt=part(7, 2, 3, top, sibling),
            hlb=part(8, 2, 3, bot, sibling),
            hrb=part(9, 6, 7, bot, sibling),
            hrt=part(10, 6, 7, top, sibling),
            hft=part(11, 4, 5, top, sibling),
            hfb=part(12, 4, 5, bot, sibling),
        )

    def spread_first(cp):
        for name in ("rt", "lb", "rb", "lt", "sib"):
            cp[name].start()

    def spread_second(cp):
        for name, fwd, hand in (("rt", "ft", "hlt"), ("lb", "fb", "hrb"), ("rb", None, "hlb"), ("lt", None, "hrt")):
            cp[name].wait_recv()
            if fwd:
                cp[fwd].start()
            cp[hand].start()

    def spread_third(cp):
        for name, hand in (("ft", "hft"), ("fb", "hfb")):
            cp[name].wait_recv()
            cp[hand].start()

    f_cp = spread(feats, fs_sem, fr_sem)
    spread_first(f_cp)
    spread_second(f_cp)

    def squares(i):
        v = feats[i].astype(F32)
        v = v * v
        return v[:, :128] + v[:, 128:]

    f_cp["sib"].wait_recv()
    total = squares(0) + squares(1) + squares(2) + squares(6)
    for name in ("hlt", "hlb", "hrb", "hrt"):
        f_cp[name].wait_recv()
    total = total + squares(3) + squares(7)
    spread_third(f_cp)
    total = total + squares(4)
    for name in ("hft", "hfb"):
        f_cp[name].wait_recv()
    total = total + squares(5)
    inv = lax.rsqrt(jnp.sum(total, axis=-1, keepdims=True) * (1.0 / D) + EPS)

    for i in range(8):
        dy, dc = i // 2, i % 2
        src = ((y - dy + NY) % NY) * 2 + (c if dc == 0 else 1 - c)
        cols = pl.ds(pl.multiple_of(src * COLS, COLS), COLS)
        normed[:, cols] = (feats[i].astype(F32) * inv * gain_ref[:, cols]).astype(BF16)

    def rms(v, g):
        return (v * lax.rsqrt(jnp.mean(v * v, axis=-1, keepdims=True) + EPS) * g[...]).astype(BF16)

    cos_t = trig[0:32, :]
    sin_t = trig[32:64, :]

    def rotate_t(v):
        a, b = v[:32], v[32:]
        return jnp.concatenate([a * cos_t - b * sin_t, b * cos_t + a * sin_t], axis=0)

    loads[L_KVL].wait()
    loads[L_R].wait()
    loads[L_KU].wait()
    loads[L_VU].wait()
    loads[L_K].wait()
    loads[L_V].wait()
    lkv = rms(dot(normed[...], wkvl[...]), kvgain_ref)
    kbuf[0] = dot(lkv, wku[...]).astype(BF16)
    rvbuf[0, 64:192] = jnp.transpose(dot(lkv, wvu[...])).astype(BF16)
    rkv = contract(normed[...], wrkv[...], 1, 1)
    rvbuf[0, 0:64] = rotate_t(jnp.transpose(rkv[:, 0:64])).astype(BF16)
    ext[WINDOW:, :] = rkv[:, 64:192].astype(BF16)

    def k_copy(i, src, dst, dev):
        return remote(kbuf.at[src], kbuf.at[dst], ks_sem.at[i], kr_sem.at[i], dev)

    def v_copy(i, src, dst, dev):
        return remote(rvbuf.at[src], rvbuf.at[dst], vs_sem.at[i], vr_sem.at[i], dev)

    up, down = z_peer(1), z_peer(-1)
    ups = [(0, 0, 1), (1, 1, 2), (2, 2, 3)]
    downs = [(3, 0, 4), (4, 4, 5), (5, 5, 6)]
    k_up = [k_copy(*t, up) for t in ups]
    v_up = [v_copy(*t, up) for t in ups]
    k_dn = [k_copy(*t, down) for t in downs]
    v_dn = [v_copy(*t, down) for t in downs]
    k_far = k_copy(6, 6, 7, down)
    v_far = v_copy(6, 3, 7, up)
    k_up[0].start()
    k_dn[0].start()
    v_up[0].start()
    v_dn[0].start()

    tail = remote(ext.at[pl.ds(ROWS, WINDOW)], ext.at[pl.ds(0, WINDOW)], ts_sem, tr_sem, sp_peer(1))
    tail.start()

    loads[L_QL].wait()
    loads[L_QC].wait()
    loads[L_QR].wait()
    lq = rms(dot(normed[...], wql[...]), qgain_ref)
    qbuf[0:128, 0:ROWS] = jnp.transpose(dot(lq, wqc[...])).astype(BF16)
    qbuf[128:192, 0:ROWS] = rotate_t(contract(wqrt[...], lq, 1, 1)).astype(BF16)
    slots = [pl.ds(d * ROWS, ROWS) for d in range(NX)]
    q_half = (pl.ds(0, 96), pl.ds(96, 96))

    def q_copy(i, rows, src, dst, by):
        return remote(
            qbuf.at[rows, slots[src]], qbuf.at[rows, slots[dst]], qs_sem.at[i], qr_sem.at[i], x_peer(by)
        )

    q_all = pl.ds(0, NOPE + ROPE)
    q_cp = [q_copy(0, q_all, 0, 1, 1), q_copy(1, q_all, 0, 3, -1)]
    q_fwd = [q_copy(2, q_half[0], 1, 2, 1), q_copy(3, q_half[1], 3, 2, -1)]
    for cp in q_cp:
        cp.start()

    branch = []
    for slot in range(1, NTP):
        dy, dc = slot // 2, slot % 2
        peer = ((y + dy) % NY) * 2 + (c if dc == 0 else 1 - c)
        cols = pl.ds(pl.multiple_of(peer * COLS, COLS), COLS)
        i, j = slot - 1, slot + 6
        branch.append(remote(wbw_h.at[:, cols], colw.at[slot], bs_sem.at[i], br_sem.at[i], (sp, peer)))
        branch.append(remote(wbl_h.at[:, cols], coll.at[slot], bs_sem.at[j], br_sem.at[j], (sp, peer)))
    for cp in branch:
        cp.start()

    loads[L_Q].wait()
    qwin[...] = dot(normed[...], wq[...]).astype(BF16)
    loads[L_GW].wait()
    loads[L_GL].wait()
    gatew[...] = jax.nn.sigmoid(dot(normed[...], wgw[...]))
    gatel[...] = jax.nn.sigmoid(dot(normed[...], wgl[...]))

    def windowed():
        tail.wait_recv()
        ki = lax.broadcasted_iota(jnp.int32, (256, 256), 0)
        ci = lax.broadcasted_iota(jnp.int32, (256, 256), 1)
        offset = jnp.where(ci < 128, ci, ci - 128) + WINDOW - ki
        band = (offset >= 0) & (offset < WINDOW)
        first = lax.broadcasted_iota(jnp.int32, (1, 256), 1) < 128
        sink = jnp.where(first, sink_ref[0], sink_ref[1])
        for n in range(ROWS // WINDOW):
            lo = n * WINDOW
            q2 = jnp.concatenate([qwin[lo : lo + 128, 0:64], qwin[lo : lo + 128, 64:128]], axis=0)
            kv = ext[lo : lo + 256, :]
            s = contract(kv[:, 0:64], q2, 1, 1) * HEAD ** (-0.5)
            valid = band & (sp * ROWS + lo - WINDOW + ki >= 0)
            s = jnp.where(valid, s, NEGATIVE)
            peak = jnp.maximum(jnp.max(s, axis=0, keepdims=True), sink)
            w = jnp.where(valid, jnp.exp(s - peak), 0.0)
            den = jnp.sum(w, axis=0, keepdims=True) + jnp.exp(sink - peak)
            p = (w / den).astype(BF16)
            o = contract(p, kv[:, 64:128], 0, 0).astype(BF16)
            wout[0, lo : lo + 128, :] = jnp.concatenate([o[:128], o[128:]], axis=1)
        spread_first(w_cp)

    w_cp = spread(wout, ws_sem, wr_sem)

    m_s[...] = jnp.full((1, NX * ROWS), NEGATIVE, F32)
    l_s[...] = jnp.zeros((1, NX * ROWS), F32)
    acc[...] = jnp.zeros((VDIM, NX * ROWS), F32)

    def tile(keys, vals, cols, masked):
        s = dot(keys, qbuf[:, cols])
        if masked:
            kpos = lax.broadcasted_iota(jnp.int32, (ROWS, ROWS), 0)
            qpos = lax.broadcasted_iota(jnp.int32, (ROWS, ROWS), 1)
            s = jnp.where(kpos <= qpos, s, NEGATIVE)
        m_old = m_s[:, cols]
        m_new = jnp.maximum(m_old, jnp.max(s, axis=0, keepdims=True))
        p = jnp.exp2((s - m_new) * SOFT)
        alpha = jnp.exp2((m_old - m_new) * SOFT)
        m_s[:, cols] = m_new
        l_s[:, cols] = l_s[:, cols] * alpha + jnp.sum(p, axis=0, keepdims=True)
        acc[:, cols] = acc[:, cols] * alpha + dot(vals, p.astype(BF16))

    def block(slot):
        keys = jnp.concatenate([kbuf[slot], jnp.transpose(rvbuf[slot, 0:64])], axis=1)
        return keys, rvbuf[slot, 64:192]

    def whole(slot, useful):
        @pl.when(useful)
        def _():
            keys, vals = block(slot)
            tile(keys, vals, pl.ds(0, NX * ROWS), False)

    def own():
        keys, vals = block(0)
        tile(keys, vals, slots[0], True)
        for d in range(1, NX):

            @pl.when(d > x)
            def _():
                tile(keys, vals, slots[d], False)

    def relay(arrived, after):
        for cp, nxt in zip(arrived, after):
            cp.wait_recv()
            if nxt is not None:
                nxt.start()

    relay((k_up[0], k_dn[0]), (k_up[1], k_dn[1]))
    relay((v_up[0], v_dn[0]), (v_up[1], v_dn[1]))
    relay(q_cp, q_fwd)
    windowed()
    relay((k_up[1], k_dn[1]), (k_up[2], k_dn[2]))
    relay(q_fwd, (None, None))
    own()
    relay((v_up[1], v_dn[1]), (v_up[2], v_dn[2]))
    whole(1, z >= 1)
    relay((k_up[2], k_dn[2]), (None, k_far))
    whole(4, z >= 7)
    spread_second(w_cp)
    relay((v_up[2], v_dn[2]), (v_far, None))
    whole(2, z >= 2)
    whole(5, z >= 6)
    spread_third(w_cp)
    whole(3, z >= 3)
    whole(6, z >= 5)
    relay((k_far, v_far), (None, None))
    whole(7, z >= 4)

    o_cp = []
    for d in range(1, NX):
        o_send[d - 1] = acc[:, slots[d]].astype(BF16)
        st_send[d - 1, 0:1] = m_s[:, slots[d]]
        st_send[d - 1, 1:2] = l_s[:, slots[d]]
        o_cp.append(remote(o_send.at[d - 1], o_recv.at[d - 1], os_sem.at[d - 1], or_sem.at[d - 1], x_peer(-d)))
        o_cp.append(remote(st_send.at[d - 1], st_recv.at[d - 1], ss_sem.at[d - 1], sr_sem.at[d - 1], x_peer(-d)))
    for cp in o_cp:
        cp.start()

    for cp in branch:
        cp.wait_recv()
    loads[L_BW].wait()
    loads[L_BL].wait()
    for name in ("sib", "hlt", "hlb", "hrb", "hrt", "hft", "hfb"):
        w_cp[name].wait_recv()
    allw = jnp.concatenate([wout[d] for d in range(NTP)], axis=1)
    gatew[...] = gatew[...] * dot(allw, colw[...].reshape(NTP * 128, COLS))

    for cp in o_cp:
        cp.wait_recv()
    ms = [m_s[:, slots[0]]] + [st_recv[d, 0:1] for d in range(3)]
    ls = [l_s[:, slots[0]]] + [st_recv[d, 1:2] for d in range(3)]
    top_m = jnp.maximum(jnp.maximum(ms[0], ms[1]), jnp.maximum(ms[2], ms[3]))
    ws = [jnp.exp2((m - top_m) * SOFT) for m in ms]
    den = ls[0] * ws[0] + ls[1] * ws[1] + ls[2] * ws[2] + ls[3] * ws[3]
    o = acc[:, slots[0]] * ws[0]
    for d in range(3):
        o = o + o_recv[d].astype(F32) * ws[d + 1]
    lat[0] = jnp.transpose(o / den).astype(BF16)
    l_cp = spread(lat, ls_sem, lr_sem)
    spread_first(l_cp)
    spread_second(l_cp)
    l_cp["sib"].wait_recv()

    def branch_part(first, count):
        rows = jnp.concatenate([lat[i] for i in range(first, first + count)], axis=1)
        return dot(rows, coll[first : first + count].reshape(count * 128, COLS))

    mixed = branch_part(0, 2)
    spread_third(l_cp)
    for name in ("hlt", "hlb", "hrb", "hrt"):
        l_cp[name].wait_recv()
    mixed = mixed + branch_part(2, 2) + branch_part(6, 2)
    for name in ("hft", "hfb"):
        l_cp[name].wait_recv()
    mixed = mixed + branch_part(4, 2)
    out_ref[...] = (gatew[...] + gatel[...] * mixed).astype(BF16)

    sent = list(f_cp.values()) + list(w_cp.values()) + list(l_cp.values())
    sent += branch + k_up + k_dn + v_up + v_dn + [k_far, v_far] + q_cp + q_fwd + [tail] + o_cp
    for cp in sent:
        cp.wait_send()


def on_device(
    features, norm_gain, w_query, w_key, w_value, head_sinks, w_query_latent, w_kv_latent, w_rope_key,
    query_latent_gain, kv_latent_gain, w_query_content, w_query_rotary, w_key_up, w_value_up,
    w_branch_window, w_branch_latent, w_gate_window, w_gate_latent,
):
    vmem = pl.BlockSpec(memory_space=pltpu.VMEM)
    anyspace = pl.BlockSpec(memory_space=pl.ANY)
    smem = pl.BlockSpec(memory_space=pltpu.SMEM)
    dma = pltpu.SemaphoreType.DMA
    scratch = [
        pltpu.VMEM((8, ROWS, COLS), BF16),
        pltpu.VMEM((ROWS, D), BF16),
    ]
    weights = [
        w_query, w_key.T, w_value.T, w_query_latent, w_kv_latent, w_rope_key.T, w_query_content, w_query_rotary.T,
        w_key_up, w_value_up, w_branch_window, w_branch_latent, w_gate_window, w_gate_latent,
    ]
    shapes = [
        (D, 128), (192, D), (D, LATENT), (D, LATENT), (LATENT, NOPE), (ROPE, LATENT), (LATENT, NOPE), (LATENT, VDIM),
        (D, COLS), (D, COLS),
    ]
    scratch += [pltpu.VMEM(shape, BF16) for shape in shapes] + [pltpu.VMEM((ROPE, ROWS), F32)]
    scratch += [
        pltpu.VMEM((NTP, 128, COLS), BF16),
        pltpu.VMEM((NTP, 128, COLS), BF16),
        pltpu.VMEM((8, ROWS, NOPE), BF16),
        pltpu.VMEM((8, ROPE + VDIM, ROWS), BF16),
        pltpu.VMEM((NOPE + ROPE, NX * ROWS), BF16),
        pltpu.VMEM((ROWS + WINDOW, 128), BF16),
        pltpu.VMEM((ROWS, 128), BF16),
        pltpu.VMEM((ROWS, COLS), F32),
        pltpu.VMEM((ROWS, COLS), F32),
        pltpu.VMEM((1, NX * ROWS), F32),
        pltpu.VMEM((1, NX * ROWS), F32),
        pltpu.VMEM((VDIM, NX * ROWS), F32),
        pltpu.VMEM((NX - 1, VDIM, ROWS), BF16),
        pltpu.VMEM((NX - 1, 2, ROWS), F32),
        pltpu.VMEM((NX - 1, VDIM, ROWS), BF16),
        pltpu.VMEM((NX - 1, 2, ROWS), F32),
        pltpu.VMEM((NTP, ROWS, 128), BF16),
        pltpu.VMEM((NTP, ROWS, 128), BF16),
    ]
    scratch += [
        dma((15,)), dma((13,)), dma((13,)), dma((7,)), dma((7,)), dma((7,)), dma((7,)),
        dma((4,)), dma((4,)), dma(()), dma(()), dma((14,)), dma((14,)),
        dma((3,)), dma((3,)), dma((3,)), dma((3,)), dma((13,)), dma((13,)), dma((13,)), dma((13,)),
    ]
    return pl.pallas_call(
        layer,
        out_shape=pltpu.VMEM((ROWS, COLS), BF16),
        in_specs=[anyspace, vmem, vmem, vmem, smem] + [anyspace] * 14,
        out_specs=vmem,
        scratch_shapes=scratch,
        compiler_params=pltpu.CompilerParams(
            collective_id=0, has_side_effects=True, vmem_limit_bytes=60 * 1024 * 1024
        ),
    )(
        features, norm_gain.reshape(1, D), query_latent_gain.reshape(1, LATENT),
        kv_latent_gain.reshape(1, LATENT), head_sinks, *weights,
    )


def solution(mesh):
    return jax.shard_map(
        on_device,
        mesh=mesh,
        in_specs=(
            P("sp", "tp"), P(), P(None, "tp"), P(None, "tp"), P(None, "tp"), P("tp"), P(), P(), P(), P(), P(),
            P(None, "tp"), P(None, "tp"), P(None, "tp"), P(None, "tp"), P("tp", None), P("tp", None),
            P(None, "tp"), P(None, "tp"),
        ),
        out_specs=P("sp", "tp"),
        check_vma=False,
    )
```

```python
import functools
import math

import jax
import jax.numpy as jnp
from jax import lax
from jax.experimental import pallas as pl
from jax.experimental.pallas import tpu as pltpu
from jax.sharding import PartitionSpec as P

D = 2048
HEAD = 64
WINDOW = 128
NOPE = 128
ROPE = 64
VDIM = 128
LATENT = 512
ROWS = 384
COLS = 256
NX = 4
NY = 4
NZ = 8
NTP = 8
NSP = 32
EPS = 1e-06
THETA = 10000.0
NEGATIVE = -1e30
SOFT = (NOPE + ROPE) ** (-0.5) * math.log2(math.e)
MESH = pl.DeviceIdType.MESH
F32 = jnp.float32
BF16 = jnp.bfloat16


def dot(a, b):
    return jnp.dot(a, b, preferred_element_type=F32)


def contract(a, b, da, db):
    return lax.dot_general(a, b, (((da,), (db,)), ((), ())), preferred_element_type=F32)


def layer(
    x_ref, gain_ref, qgain_ref, kvgain_ref, sink_ref,
    wq_h, wkt_h, wvt_h, wql_h, wkvl_h, wrt_h, wqc_h, wqrt_h, wku_h, wvu_h, wbw_h, wbl_h, wgw_h, wgl_h,
    out_ref,
    feats, normed,
    wq, wrkv, wql, wkvl, wqc, wqrt, wku, wvu, wgw, wgl, trig,
    colw, coll, kbuf, rvbuf, qbuf, ext, qwin, gatew, gatel,
    m_s, l_s, acc, o_send, st_send, o_recv, st_recv, wout, lat,
    w_sem, fs_sem, fr_sem, ks_sem, kr_sem, vs_sem, vr_sem, qs_sem, qr_sem, ts_sem, tr_sem,
    bs_sem, br_sem, os_sem, or_sem, ss_sem, sr_sem, ws_sem, wr_sem, ls_sem, lr_sem,
):
    sp = lax.axis_index("sp")
    tp = lax.axis_index("tp")
    z = sp // NX
    x = sp % NX
    y = tp // 2
    c = tp % 2

    def z_peer(by):
        return (((z + by + NZ) % NZ) * NX + x, tp)

    def x_peer(by):
        return (z * NX + (x + by + NX) % NX, tp)

    def y_peer(by):
        return (sp, ((y + by + NY) % NY) * 2 + c)

    def tp_peer(by):
        return (sp, (tp + by + NTP) % NTP)

    def sp_peer(by):
        return ((sp + by + NSP) % NSP, tp)

    sibling = (sp, tp + 1 - 2 * c)

    def remote(src, dst, ssem, rsem, dev):
        return pltpu.make_async_remote_copy(
            src_ref=src, dst_ref=dst, send_sem=ssem, recv_sem=rsem, device_id=dev, device_id_type=MESH
        )

    own_cols = pl.ds(pl.multiple_of(tp * COLS, COLS), COLS)
    pairs = [
        (wkvl_h, wkvl), (wrt_h, wrkv.at[pl.ds(0, 64)]), (wku_h, wku), (wvu_h, wvu), (wql_h, wql), (wqc_h, wqc),
        (wqrt_h, wqrt), (wq_h, wq), (wkt_h, wrkv.at[pl.ds(64, 64)]), (wvt_h, wrkv.at[pl.ds(128, 64)]),
        (wgw_h, wgw), (wgl_h, wgl),
        (wbw_h.at[:, own_cols], colw.at[0]), (wbl_h.at[:, own_cols], coll.at[0]),
        (x_ref, feats.at[0]),
    ]
    loads = [pltpu.make_async_copy(a, b, w_sem.at[i]) for i, (a, b) in enumerate(pairs)]
    (L_KVL, L_R, L_KU, L_VU, L_QL, L_QC, L_QR, L_Q, L_K, L_V, L_GW, L_GL, L_BW, L_BL, L_X) = range(15)
    loads[L_X].start()
    for i in range(14):
        loads[i].start()

    barrier = pltpu.get_barrier_semaphore()
    partners = [z_peer(1), z_peer(-1), sp_peer(1), sp_peer(-1)]
    partners += [x_peer(d) for d in range(1, NX)]
    partners += [tp_peer(d) for d in range(1, NTP)]
    for dev in partners:
        pl.semaphore_signal(barrier, inc=1, device_id=dev, device_id_type=MESH)
    spots = lax.broadcasted_iota(jnp.int32, (ROPE // 2, ROWS), 1) + sp * ROWS
    freq_at = lax.broadcasted_iota(jnp.int32, (ROPE // 2, ROWS), 0)
    frequencies = jnp.exp(freq_at.astype(F32) * (-math.log(THETA) / (ROPE // 2)))
    angles = spots.astype(F32) * frequencies
    trig[0:32, :] = jnp.cos(angles)
    trig[32:64, :] = jnp.sin(angles)
    pl.semaphore_wait(barrier, len(partners))
    loads[L_X].wait()

    def spread(buf, ssem, rsem, lo=0, count=ROWS, first=0):
        half = count // 2
        every, top, bot = pl.ds(lo, count), pl.ds(lo, half), pl.ds(lo + half, half)

        def part(i, src, dst, rows, dev):
            return remote(buf.at[src, rows], buf.at[dst, rows], ssem.at[first + i], rsem.at[first + i], dev)

        return dict(
            sib=part(0, 0, 1, every, sibling),
            rt=part(1, 0, 2, top, y_peer(1)),
            rb=part(2, 0, 2, bot, y_peer(1)),
            lb=part(3, 0, 6, bot, y_peer(-1)),
            lt=part(4, 0, 6, top, y_peer(-1)),
            ft=part(5, 2, 4, top, y_peer(1)),
            fb=part(6, 6, 4, bot, y_peer(-1)),
            hlt=part(7, 2, 3, top, sibling),
            hlb=part(8, 2, 3, bot, sibling),
            hrb=part(9, 6, 7, bot, sibling),
            hrt=part(10, 6, 7, top, sibling),
            hft=part(11, 4, 5, top, sibling),
            hfb=part(12, 4, 5, bot, sibling),
        )

    def spread_first(cp):
        for name in ("rt", "lb", "rb", "lt", "sib"):
            cp[name].start()

    def spread_second(cp):
        for name, fwd, hand in (("rt", "ft", "hlt"), ("lb", "fb", "hrb"), ("rb", None, "hlb"), ("lt", None, "hrt")):
            cp[name].wait_recv()
            if fwd:
                cp[fwd].start()
            cp[hand].start()

    def spread_third(cp):
        for name, hand in (("ft", "hft"), ("fb", "hfb")):
            cp[name].wait_recv()
            cp[hand].start()

    f_cp = spread(feats, fs_sem, fr_sem)
    spread_first(f_cp)
    spread_second(f_cp)

    def squares(i):
        v = feats[i].astype(F32)
        v = v * v
        return v[:, :128] + v[:, 128:]

    f_cp["sib"].wait_recv()
    total = squares(0) + squares(1) + squares(2) + squares(6)
    for name in ("hlt", "hlb", "hrb", "hrt"):
        f_cp[name].wait_recv()
    total = total + squares(3) + squares(7)
    spread_third(f_cp)
    total = total + squares(4)
    for name in ("hft", "hfb"):
        f_cp[name].wait_recv()
    total = total + squares(5)
    inv = lax.rsqrt(jnp.sum(total, axis=-1, keepdims=True) * (1.0 / D) + EPS)

    for i in range(8):
        dy, dc = i // 2, i % 2
        src = ((y - dy + NY) % NY) * 2 + (c if dc == 0 else 1 - c)
        cols = pl.ds(pl.multiple_of(src * COLS, COLS), COLS)
        normed[:, cols] = (feats[i].astype(F32) * inv * gain_ref[:, cols]).astype(BF16)

    def rms(v, g):
        return (v * lax.rsqrt(jnp.mean(v * v, axis=-1, keepdims=True) + EPS) * g[...]).astype(BF16)

    cos_t = trig[0:32, :]
    sin_t = trig[32:64, :]

    def rotate_t(v):
        a, b = v[:32], v[32:]
        return jnp.concatenate([a * cos_t - b * sin_t, b * cos_t + a * sin_t], axis=0)

    loads[L_KVL].wait()
    loads[L_R].wait()
    loads[L_KU].wait()
    loads[L_VU].wait()
    loads[L_K].wait()
    loads[L_V].wait()
    lkv = rms(dot(normed[...], wkvl[...]), kvgain_ref)
    kbuf[0] = dot(lkv, wku[...]).astype(BF16)
    rvbuf[0, 64:192] = jnp.transpose(dot(lkv, wvu[...])).astype(BF16)
    rkv = contract(normed[...], wrkv[...], 1, 1)
    rvbuf[0, 0:64] = rotate_t(jnp.transpose(rkv[:, 0:64])).astype(BF16)
    ext[WINDOW:, :] = rkv[:, 64:192].astype(BF16)

    def k_copy(i, src, dst, dev):
        return remote(kbuf.at[src], kbuf.at[dst], ks_sem.at[i], kr_sem.at[i], dev)

    def v_copy(i, src, dst, dev):
        return remote(rvbuf.at[src], rvbuf.at[dst], vs_sem.at[i], vr_sem.at[i], dev)

    up, down = z_peer(1), z_peer(-1)
    ups = [(0, 0, 1), (1, 1, 2), (2, 2, 3)]
    downs = [(3, 0, 4), (4, 4, 5), (5, 5, 6)]
    k_up = [k_copy(*t, up) for t in ups]
    v_up = [v_copy(*t, up) for t in ups]
    k_dn = [k_copy(*t, down) for t in downs]
    v_dn = [v_copy(*t, down) for t in downs]
    k_far = k_copy(6, 6, 7, down)
    v_far = v_copy(6, 3, 7, up)

    def up_got(k):
        return z >= k

    def up_go(k):
        return (z >= k) & (z < NZ - 1)

    def k_down(k):
        return (z + k) % NZ <= 3

    def v_down(k):
        return (z + k) % NZ <= 2

    def when_start(cond, cp):
        @pl.when(cond)
        def _():
            cp.start()

    def when_recv(cond, cp):
        @pl.when(cond)
        def _():
            cp.wait_recv()

    def when_sent(cond, cp):
        @pl.when(cond)
        def _():
            cp.wait_send()

    when_start(up_go(0), k_up[0])
    when_start(k_down(0), k_dn[0])
    when_start(up_go(0), v_up[0])
    when_start(v_down(0), v_dn[0])

    tail = remote(ext.at[pl.ds(ROWS, WINDOW)], ext.at[pl.ds(0, WINDOW)], ts_sem, tr_sem, sp_peer(1))
    tail.start()

    loads[L_QL].wait()
    loads[L_QC].wait()
    loads[L_QR].wait()
    lq = rms(dot(normed[...], wql[...]), qgain_ref)
    qbuf[0:128, 0:ROWS] = jnp.transpose(dot(lq, wqc[...])).astype(BF16)
    qbuf[128:192, 0:ROWS] = rotate_t(contract(wqrt[...], lq, 1, 1)).astype(BF16)
    slots = [pl.ds(d * ROWS, ROWS) for d in range(NX)]
    q_half = (pl.ds(0, 96), pl.ds(96, 96))

    def q_copy(i, rows, src, dst, by):
        return remote(
            qbuf.at[rows, slots[src]], qbuf.at[rows, slots[dst]], qs_sem.at[i], qr_sem.at[i], x_peer(by)
        )

    q_all = pl.ds(0, NOPE + ROPE)
    q_cp = [q_copy(0, q_all, 0, 1, 1), q_copy(1, q_all, 0, 3, -1)]
    q_fwd = [q_copy(2, q_half[0], 1, 2, 1), q_copy(3, q_half[1], 3, 2, -1)]
    for cp in q_cp:
        cp.start()

    branch = []
    for slot in range(1, NTP):
        dy, dc = slot // 2, slot % 2
        peer = ((y + dy) % NY) * 2 + (c if dc == 0 else 1 - c)
        cols = pl.ds(pl.multiple_of(peer * COLS, COLS), COLS)
        i, j = slot - 1, slot + 6
        branch.append(remote(wbw_h.at[:, cols], colw.at[slot], bs_sem.at[i], br_sem.at[i], (sp, peer)))
        branch.append(remote(wbl_h.at[:, cols], coll.at[slot], bs_sem.at[j], br_sem.at[j], (sp, peer)))
    for cp in branch:
        cp.start()

    loads[L_Q].wait()
    qwin[...] = dot(normed[...], wq[...]).astype(BF16)
    loads[L_GW].wait()
    loads[L_GL].wait()
    gatew[...] = jax.nn.sigmoid(dot(normed[...], wgw[...]))
    gatel[...] = jax.nn.sigmoid(dot(normed[...], wgl[...]))

    def windowed():
        tail.wait_recv()
        ki = lax.broadcasted_iota(jnp.int32, (256, 256), 0)
        ci = lax.broadcasted_iota(jnp.int32, (256, 256), 1)
        offset = jnp.where(ci < 128, ci, ci - 128) + WINDOW - ki
        band = (offset >= 0) & (offset < WINDOW)
        first = lax.broadcasted_iota(jnp.int32, (1, 256), 1) < 128
        sink = jnp.where(first, sink_ref[0], sink_ref[1])
        for n in range(ROWS // WINDOW):
            lo = n * WINDOW
            q2 = jnp.concatenate([qwin[lo : lo + 128, 0:64], qwin[lo : lo + 128, 64:128]], axis=0)
            kv = ext[lo : lo + 256, :]
            s = contract(kv[:, 0:64], q2, 1, 1) * HEAD ** (-0.5)
            valid = band & (sp * ROWS + lo - WINDOW + ki >= 0)
            s = jnp.where(valid, s, NEGATIVE)
            peak = jnp.maximum(jnp.max(s, axis=0, keepdims=True), sink)
            w = jnp.where(valid, jnp.exp(s - peak), 0.0)
            den = jnp.sum(w, axis=0, keepdims=True) + jnp.exp(sink - peak)
            p = (w / den).astype(BF16)
            o = contract(p, kv[:, 64:128], 0, 0).astype(BF16)
            wout[0, lo : lo + 128, :] = jnp.concatenate([o[:128], o[128:]], axis=1)
        spread_first(w_cp)

    w_cp = spread(wout, ws_sem, wr_sem)

    m_s[...] = jnp.full((1, NX * ROWS), NEGATIVE, F32)
    l_s[...] = jnp.zeros((1, NX * ROWS), F32)
    acc[...] = jnp.zeros((VDIM, NX * ROWS), F32)

    def tile(keys, vals, cols, masked):
        s = dot(keys, qbuf[:, cols])
        if masked:
            kpos = lax.broadcasted_iota(jnp.int32, (ROWS, ROWS), 0)
            qpos = lax.broadcasted_iota(jnp.int32, (ROWS, ROWS), 1)
            s = jnp.where(kpos <= qpos, s, NEGATIVE)
        m_old = m_s[:, cols]
        m_new = jnp.maximum(m_old, jnp.max(s, axis=0, keepdims=True))
        p = jnp.exp2((s - m_new) * SOFT)
        alpha = jnp.exp2((m_old - m_new) * SOFT)
        m_s[:, cols] = m_new
        l_s[:, cols] = l_s[:, cols] * alpha + jnp.sum(p, axis=0, keepdims=True)
        acc[:, cols] = acc[:, cols] * alpha + dot(vals, p.astype(BF16))

    def block(slot):
        keys = jnp.concatenate([kbuf[slot], jnp.transpose(rvbuf[slot, 0:64])], axis=1)
        return keys, rvbuf[slot, 64:192]

    def whole(slot, useful):
        @pl.when(useful)
        def _():
            keys, vals = block(slot)
            tile(keys, vals, pl.ds(0, NX * ROWS), False)

    def own():
        keys, vals = block(0)
        tile(keys, vals, slots[0], True)
        for d in range(1, NX):

            @pl.when(d > x)
            def _():
                tile(keys, vals, slots[d], False)

    def relay_k(k):
        when_recv(up_got(k), k_up[k - 1])
        if k < 3:
            when_start(up_go(k), k_up[k])
        when_recv(k_down(k), k_dn[k - 1])
        when_start(k_down(k), k_dn[k] if k < 3 else k_far)

    def relay_v(k):
        when_recv(up_got(k), v_up[k - 1])
        when_start(up_go(k), v_up[k] if k < 3 else v_far)
        when_recv(v_down(k), v_dn[k - 1])
        if k < 3:
            when_start(v_down(k), v_dn[k])

    relay_k(1)
    relay_v(1)
    for cp, nxt in zip(q_cp, q_fwd):
        cp.wait_recv()
        nxt.start()
    windowed()
    relay_k(2)
    for cp in q_fwd:
        cp.wait_recv()
    own()
    relay_v(2)
    whole(1, z >= 1)
    relay_k(3)
    whole(4, z >= 7)
    spread_second(w_cp)
    relay_v(3)
    whole(2, z >= 2)
    whole(5, z >= 6)
    spread_third(w_cp)
    whole(3, z >= 3)
    whole(6, z >= 5)
    when_recv(z >= 4, k_far)
    when_recv(z >= 4, v_far)
    whole(7, z >= 4)

    pieces = [pl.ds(p * 128, 128) for p in range(3)]
    st_cp, o_cp = [], [[], [], []]
    for d in (2, 1, 3):
        st_send[d - 1, 0:1] = m_s[:, slots[d]]
        st_send[d - 1, 1:2] = l_s[:, slots[d]]
        st_cp.append(remote(st_send.at[d - 1], st_recv.at[d - 1], ss_sem.at[d - 1], sr_sem.at[d - 1], x_peer(-d)))
    for cp in st_cp:
        cp.start()
    for p in range(3):
        for d in (2, 1, 3):
            i = (d - 1) * 3 + p
            o_send[i] = acc[:, pl.ds(d * ROWS + p * 128, 128)].astype(BF16)
            o_cp[p].append(remote(o_send.at[i], o_recv.at[i], os_sem.at[i], or_sem.at[i], x_peer(-d)))
            o_cp[p][-1].start()

    for cp in branch:
        cp.wait_recv()
    loads[L_BW].wait()
    loads[L_BL].wait()
    for name in ("sib", "hlt", "hlb", "hrb", "hrt", "hft", "hfb"):
        w_cp[name].wait_recv()
    allw = jnp.concatenate([wout[d] for d in range(NTP)], axis=1)
    gatew[...] = gatew[...] * dot(allw, colw[...].reshape(NTP * 128, COLS))

    l_cp = [spread(lat, ls_sem, lr_sem, p * 128, 128, p * 13) for p in range(3)]
    for cp in st_cp:
        cp.wait_recv()
    for p, cols in enumerate(pieces):
        for cp in o_cp[p]:
            cp.wait_recv()
        ms = [m_s[:, cols]] + [st_recv[d, 0:1, cols] for d in range(3)]
        ls = [l_s[:, cols]] + [st_recv[d, 1:2, cols] for d in range(3)]
        top_m = jnp.maximum(jnp.maximum(ms[0], ms[1]), jnp.maximum(ms[2], ms[3]))
        ws = [jnp.exp2((m - top_m) * SOFT) for m in ms]
        den = ls[0] * ws[0] + ls[1] * ws[1] + ls[2] * ws[2] + ls[3] * ws[3]
        o = acc[:, cols] * ws[0]
        for d in range(3):
            o = o + o_recv[d * 3 + p].astype(F32) * ws[d + 1]
        lat[0, cols] = jnp.transpose(o / den).astype(BF16)
        spread_first(l_cp[p])
    for cp in l_cp:
        spread_second(cp)
    for cp in l_cp:
        cp["sib"].wait_recv()

    def branch_part(first, count):
        rows = jnp.concatenate([lat[i] for i in range(first, first + count)], axis=1)
        return dot(rows, coll[first : first + count].reshape(count * 128, COLS))

    mixed = branch_part(0, 2)
    for cp in l_cp:
        spread_third(cp)
    for cp in l_cp:
        for name in ("hlt", "hlb", "hrb", "hrt"):
            cp[name].wait_recv()
    mixed = mixed + branch_part(2, 2) + branch_part(6, 2)
    for cp in l_cp:
        for name in ("hft", "hfb"):
            cp[name].wait_recv()
    mixed = mixed + branch_part(4, 2)
    out_ref[...] = (gatew[...] + gatel[...] * mixed).astype(BF16)

    sent = list(f_cp.values()) + list(w_cp.values()) + branch + q_cp + q_fwd + [tail] + st_cp
    for p in range(3):
        sent += list(l_cp[p].values()) + o_cp[p]
    for k in range(3):
        when_sent(up_go(k), k_up[k])
        when_sent(up_go(k), v_up[k])
        when_sent(k_down(k), k_dn[k])
        when_sent(v_down(k), v_dn[k])
    when_sent(k_down(3), k_far)
    when_sent(up_go(3), v_far)
    for cp in sent:
        cp.wait_send()


def on_device(
    features, norm_gain, w_query, w_key, w_value, head_sinks, w_query_latent, w_kv_latent, w_rope_key,
    query_latent_gain, kv_latent_gain, w_query_content, w_query_rotary, w_key_up, w_value_up,
    w_branch_window, w_branch_latent, w_gate_window, w_gate_latent,
):
    vmem = pl.BlockSpec(memory_space=pltpu.VMEM)
    anyspace = pl.BlockSpec(memory_space=pl.ANY)
    smem = pl.BlockSpec(memory_space=pltpu.SMEM)
    dma = pltpu.SemaphoreType.DMA
    scratch = [
        pltpu.VMEM((8, ROWS, COLS), BF16),
        pltpu.VMEM((ROWS, D), BF16),
    ]
    weights = [
        w_query, w_key.T, w_value.T, w_query_latent, w_kv_latent, w_rope_key.T, w_query_content, w_query_rotary.T,
        w_key_up, w_value_up, w_branch_window, w_branch_latent, w_gate_window, w_gate_latent,
    ]
    shapes = [
        (D, 128), (192, D), (D, LATENT), (D, LATENT), (LATENT, NOPE), (ROPE, LATENT), (LATENT, NOPE), (LATENT, VDIM),
        (D, COLS), (D, COLS),
    ]
    scratch += [pltpu.VMEM(shape, BF16) for shape in shapes] + [pltpu.VMEM((ROPE, ROWS), F32)]
    scratch += [
        pltpu.VMEM((NTP, 128, COLS), BF16),
        pltpu.VMEM((NTP, 128, COLS), BF16),
        pltpu.VMEM((8, ROWS, NOPE), BF16),
        pltpu.VMEM((8, ROPE + VDIM, ROWS), BF16),
        pltpu.VMEM((NOPE + ROPE, NX * ROWS), BF16),
        pltpu.VMEM((ROWS + WINDOW, 128), BF16),
        pltpu.VMEM((ROWS, 128), BF16),
        pltpu.VMEM((ROWS, COLS), F32),
        pltpu.VMEM((ROWS, COLS), F32),
        pltpu.VMEM((1, NX * ROWS), F32),
        pltpu.VMEM((1, NX * ROWS), F32),
        pltpu.VMEM((VDIM, NX * ROWS), F32),
        pltpu.VMEM((9, VDIM, 128), BF16),
        pltpu.VMEM((NX - 1, 2, ROWS), F32),
        pltpu.VMEM((9, VDIM, 128), BF16),
        pltpu.VMEM((NX - 1, 2, ROWS), F32),
        pltpu.VMEM((NTP, ROWS, 128), BF16),
        pltpu.VMEM((NTP, ROWS, 128), BF16),
    ]
    scratch += [
        dma((15,)), dma((13,)), dma((13,)), dma((7,)), dma((7,)), dma((7,)), dma((7,)),
        dma((4,)), dma((4,)), dma(()), dma(()), dma((14,)), dma((14,)),
        dma((9,)), dma((9,)), dma((3,)), dma((3,)), dma((13,)), dma((13,)), dma((39,)), dma((39,)),
    ]
    return pl.pallas_call(
        layer,
        out_shape=pltpu.VMEM((ROWS, COLS), BF16),
        in_specs=[anyspace, vmem, vmem, vmem, smem] + [anyspace] * 14,
        out_specs=vmem,
        scratch_shapes=scratch,
        compiler_params=pltpu.CompilerParams(
            collective_id=0, has_side_effects=True, vmem_limit_bytes=60 * 1024 * 1024
        ),
    )(
        features, norm_gain.reshape(1, D), query_latent_gain.reshape(1, LATENT),
        kv_latent_gain.reshape(1, LATENT), head_sinks, *weights,
    )


def solution(mesh):
    return jax.shard_map(
        on_device,
        mesh=mesh,
        in_specs=(
            P("sp", "tp"), P(), P(None, "tp"), P(None, "tp"), P(None, "tp"), P("tp"), P(), P(), P(), P(), P(),
            P(None, "tp"), P(None, "tp"), P(None, "tp"), P(None, "tp"), P("tp", None), P("tp", None),
            P(None, "tp"), P(None, "tp"),
        ),
        out_specs=P("sp", "tp"),
        check_vma=False,
    )
```

```python
import functools
import math

import jax
import jax.numpy as jnp
from jax import lax
from jax.experimental import pallas as pl
from jax.experimental.pallas import tpu as pltpu
from jax.sharding import PartitionSpec as P

D = 2048
HEAD = 64
WINDOW = 128
NOPE = 128
ROPE = 64
VDIM = 128
LATENT = 512
ROWS = 384
COLS = 256
NX = 4
NY = 4
NZ = 8
NTP = 8
NSP = 32
EPS = 1e-06
THETA = 10000.0
NEGATIVE = -1e30
SOFT = (NOPE + ROPE) ** (-0.5) * math.log2(math.e)
MESH = pl.DeviceIdType.MESH
F32 = jnp.float32
BF16 = jnp.bfloat16


def dot(a, b):
    return jnp.dot(a, b, preferred_element_type=F32)


def contract(a, b, da, db):
    return lax.dot_general(a, b, (((da,), (db,)), ((), ())), preferred_element_type=F32)


def layer(
    x_ref, gain_ref, qgain_ref, kvgain_ref, sink_ref,
    wq_h, wkt_h, wvt_h, wql_h, wkvl_h, wrt_h, wqc_h, wqrt_h, wku_h, wvu_h, wbw_h, wbl_h, wgw_h, wgl_h,
    out_ref,
    feats, normed,
    wq, wrkv, wql, wkvl, wqc, wqrt, wku, wvu, wgw, wgl, trig,
    colw, coll, kbuf, vbuf, rbuf, qbuf, ext, qwin, gatew, gatel,
    m_s, l_s, acc, o_send, st_send, o_recv, st_recv, wout, lat,
    w_sem, fs_sem, fr_sem, ks_sem, kr_sem, vs_sem, vr_sem, rs_sem, rr_sem, hs_sem, hr_sem, qs_sem, qr_sem, ts_sem, tr_sem,
    bs_sem, br_sem, os_sem, or_sem, ss_sem, sr_sem, ws_sem, wr_sem, ls_sem, lr_sem,
):
    sp = lax.axis_index("sp")
    tp = lax.axis_index("tp")
    z = sp // NX
    x = sp % NX
    y = tp // 2
    c = tp % 2

    def z_peer(by):
        return (((z + by + NZ) % NZ) * NX + x, tp)

    def x_peer(by):
        return (z * NX + (x + by + NX) % NX, tp)

    def y_peer(by):
        return (sp, ((y + by + NY) % NY) * 2 + c)

    def tp_peer(by):
        return (sp, (tp + by + NTP) % NTP)

    def sp_peer(by):
        return ((sp + by + NSP) % NSP, tp)

    sibling = (sp, tp + 1 - 2 * c)

    def remote(src, dst, ssem, rsem, dev):
        return pltpu.make_async_remote_copy(
            src_ref=src, dst_ref=dst, send_sem=ssem, recv_sem=rsem, device_id=dev, device_id_type=MESH
        )

    own_cols = pl.ds(pl.multiple_of(tp * COLS, COLS), COLS)
    pairs = [
        (wkvl_h, wkvl), (wrt_h, wrkv.at[pl.ds(0, 64)]), (wku_h, wku), (wvu_h, wvu), (wql_h, wql), (wqc_h, wqc),
        (wqrt_h, wqrt), (wq_h, wq), (wkt_h, wrkv.at[pl.ds(64, 64)]), (wvt_h, wrkv.at[pl.ds(128, 64)]),
        (wgw_h, wgw), (wgl_h, wgl),
        (wbw_h.at[:, own_cols], colw.at[0]), (wbl_h.at[:, own_cols], coll.at[0]),
        (x_ref, feats.at[0]),
    ]
    loads = [pltpu.make_async_copy(a, b, w_sem.at[i]) for i, (a, b) in enumerate(pairs)]
    (L_KVL, L_R, L_KU, L_VU, L_QL, L_QC, L_QR, L_Q, L_K, L_V, L_GW, L_GL, L_BW, L_BL, L_X) = range(15)
    loads[L_X].start()
    for i in range(14):
        loads[i].start()

    barrier = pltpu.get_barrier_semaphore()
    partners = [z_peer(1), z_peer(-1), sp_peer(1), sp_peer(-1)]
    partners += [x_peer(d) for d in range(1, NX)]
    partners += [tp_peer(d) for d in range(1, NTP)]
    for dev in partners:
        pl.semaphore_signal(barrier, inc=1, device_id=dev, device_id_type=MESH)
    spots = lax.broadcasted_iota(jnp.int32, (ROPE // 2, ROWS), 1) + sp * ROWS
    freq_at = lax.broadcasted_iota(jnp.int32, (ROPE // 2, ROWS), 0)
    frequencies = jnp.exp(freq_at.astype(F32) * (-math.log(THETA) / (ROPE // 2)))
    angles = spots.astype(F32) * frequencies
    trig[0:32, :] = jnp.cos(angles)
    trig[32:64, :] = jnp.sin(angles)
    pl.semaphore_wait(barrier, len(partners))
    loads[L_X].wait()

    def spread(buf, ssem, rsem, lo=0, count=ROWS, first=0):
        half = count // 2
        every, top, bot = pl.ds(lo, count), pl.ds(lo, half), pl.ds(lo + half, half)

        def part(i, src, dst, rows, dev):
            return remote(buf.at[src, rows], buf.at[dst, rows], ssem.at[first + i], rsem.at[first + i], dev)

        return dict(
            sib=part(0, 0, 1, every, sibling),
            rt=part(1, 0, 2, top, y_peer(1)),
            rb=part(2, 0, 2, bot, y_peer(1)),
            lb=part(3, 0, 6, bot, y_peer(-1)),
            lt=part(4, 0, 6, top, y_peer(-1)),
            ft=part(5, 2, 4, top, y_peer(1)),
            fb=part(6, 6, 4, bot, y_peer(-1)),
            hlt=part(7, 2, 3, top, sibling),
            hlb=part(8, 2, 3, bot, sibling),
            hrb=part(9, 6, 7, bot, sibling),
            hrt=part(10, 6, 7, top, sibling),
            hft=part(11, 4, 5, top, sibling),
            hfb=part(12, 4, 5, bot, sibling),
        )

    def spread_first(cp):
        for name in ("rt", "lb", "rb", "lt", "sib"):
            cp[name].start()

    def spread_second(cp):
        for name, fwd, hand in (("rt", "ft", "hlt"), ("lb", "fb", "hrb"), ("rb", None, "hlb"), ("lt", None, "hrt")):
            cp[name].wait_recv()
            if fwd:
                cp[fwd].start()
            cp[hand].start()

    def spread_third(cp):
        for name, hand in (("ft", "hft"), ("fb", "hfb")):
            cp[name].wait_recv()
            cp[hand].start()

    def direct(buf, ssem, rsem, lo=0, count=ROWS, first=0):
        rows = pl.ds(lo, count)

        def part(i, src, dst, dev):
            return remote(buf.at[src, rows], buf.at[dst, rows], ssem.at[first + i], rsem.at[first + i], dev)

        far, right, left = part(0, 0, 4, y_peer(2)), part(1, 0, 2, y_peer(1)), part(2, 0, 6, y_peer(-1))
        own = part(3, 0, 1, sibling)
        hands = [part(4, 2, 3, sibling), part(5, 6, 7, sibling), part(6, 4, 5, sibling)]
        return [far, right, left, own], hands

    def direct_first(cps):
        for cp in cps[0]:
            cp.start()

    def direct_second(cps):
        (far, right, left, own), hands = cps
        for cp, hand in zip((right, left, far), hands):
            cp.wait_recv()
            hand.start()

    f_cp = [spread(feats, fs_sem, fr_sem, p * 192, 192, p * 13) for p in range(2)]
    for cp in f_cp:
        spread_first(cp)
    for cp in f_cp:
        spread_second(cp)

    def squares(i):
        v = feats[i].astype(F32)
        v = v * v
        return v[:, :128] + v[:, 128:]

    for cp in f_cp:
        cp["sib"].wait_recv()
    total = squares(0) + squares(1) + squares(2) + squares(6)
    for cp in f_cp:
        spread_third(cp)
    for cp in f_cp:
        for name in ("hlt", "hlb", "hrb", "hrt"):
            cp[name].wait_recv()
    total = total + squares(3) + squares(7) + squares(4)
    for cp in f_cp:
        for name in ("hft", "hfb"):
            cp[name].wait_recv()
    total = total + squares(5)
    inv = lax.rsqrt(jnp.sum(total, axis=-1, keepdims=True) * (1.0 / D) + EPS)

    branch = {}
    for slot in range(1, NTP):
        dy, dc = slot // 2, slot % 2
        peer = ((y + dy) % NY) * 2 + (c if dc == 0 else 1 - c)
        cols = pl.ds(pl.multiple_of(peer * COLS, COLS), COLS)
        i, j = slot - 1, slot + 6
        branch[slot] = [
            remote(wbw_h.at[:, cols], colw.at[slot], bs_sem.at[i], br_sem.at[i], (sp, peer)),
            remote(wbl_h.at[:, cols], coll.at[slot], bs_sem.at[j], br_sem.at[j], (sp, peer)),
        ]

    def branch_start(*chosen):
        for slot in chosen:
            for cp in branch[slot]:
                cp.start()

    branch_start(1, 2, 6)

    for i in range(8):
        dy, dc = i // 2, i % 2
        src = ((y - dy + NY) % NY) * 2 + (c if dc == 0 else 1 - c)
        cols = pl.ds(pl.multiple_of(src * COLS, COLS), COLS)
        normed[:, cols] = (feats[i].astype(F32) * inv * gain_ref[:, cols]).astype(BF16)

    def rms(v, g):
        return (v * lax.rsqrt(jnp.mean(v * v, axis=-1, keepdims=True) + EPS) * g[...]).astype(BF16)

    cos_t = trig[0:32, :]
    sin_t = trig[32:64, :]

    def rotate_t(v):
        a, b = v[:32], v[32:]
        return jnp.concatenate([a * cos_t - b * sin_t, b * cos_t + a * sin_t], axis=0)

    loads[L_KVL].wait()
    loads[L_R].wait()
    loads[L_KU].wait()
    loads[L_VU].wait()
    loads[L_K].wait()
    loads[L_V].wait()
    lkv = rms(dot(normed[...], wkvl[...]), kvgain_ref)
    kbuf[0] = dot(lkv, wku[...]).astype(BF16)
    vbuf[0] = jnp.transpose(dot(lkv, wvu[...])).astype(BF16)
    rkv = contract(normed[...], wrkv[...], 1, 1)
    rbuf[0] = rotate_t(jnp.transpose(rkv[:, 0:64])).astype(BF16)
    ext[WINDOW:, :] = rkv[:, 64:192].astype(BF16)

    def k_copy(i, src, dst, dev):
        cuts = [pl.ds(h * (ROWS // 2), ROWS // 2) for h in range(2)]
        return [
            remote(kbuf.at[src, rows], kbuf.at[dst, rows], ks_sem.at[i * 2 + h], kr_sem.at[i * 2 + h], dev)
            for h, rows in enumerate(cuts)
        ]

    def v_copy(i, src, dst, dev):
        cuts = [pl.ds(h * (VDIM // 2), VDIM // 2) for h in range(2)]
        return [
            remote(vbuf.at[src, rows], vbuf.at[dst, rows], vs_sem.at[i * 2 + h], vr_sem.at[i * 2 + h], dev)
            for h, rows in enumerate(cuts)
        ]

    mine = pl.ds(pl.multiple_of(c * (ROPE // 2), ROPE // 2), ROPE // 2)

    def r_copy(i, src, dst, dev):
        return [remote(rbuf.at[src, mine], rbuf.at[dst, mine], rs_sem.at[i], rr_sem.at[i], dev)]

    r_hand = [
        [remote(rbuf.at[slot, mine], rbuf.at[slot, mine], hs_sem.at[slot - 1], hr_sem.at[slot - 1], sibling)]
        for slot in range(1, 8)
    ]
    useful = [None] + [z >= k for k in range(1, 4)] + [z + k >= NZ for k in range(1, 4)] + [z >= 4]

    up, down = z_peer(1), z_peer(-1)
    ups = [(0, 0, 1), (1, 1, 2), (2, 2, 3)]
    downs = [(3, 0, 4), (4, 4, 5), (5, 5, 6)]
    k_up = [k_copy(*t, up) for t in ups]
    v_up = [v_copy(*t, up) for t in ups]
    k_dn = [k_copy(*t, down) for t in downs]
    v_dn = [v_copy(*t, down) for t in downs]
    k_far = k_copy(6, 6, 7, down)
    r_up = [r_copy(*t, up) for t in ups]
    r_dn = [r_copy(*t, down) for t in downs]
    r_far = r_copy(6, 6, 7, down)
    v_far = v_copy(6, 3, 7, up)

    def up_got(k):
        return z >= k

    def up_go(k):
        return (z >= k) & (z < NZ - 1)

    def k_down(k):
        return (z + k) % NZ <= 3

    def v_down(k):
        return (z + k) % NZ <= 2

    def when_start(cond, cps):
        @pl.when(cond)
        def _():
            for cp in cps:
                cp.start()

    def when_recv(cond, cps):
        @pl.when(cond)
        def _():
            for cp in cps:
                cp.wait_recv()

    def when_sent(cond, cps):
        @pl.when(cond)
        def _():
            for cp in cps:
                cp.wait_send()

    when_start(up_go(0), k_up[0])
    when_start(k_down(0), k_dn[0])
    when_start(up_go(0), r_up[0])
    when_start(k_down(0), r_dn[0])
    when_start(up_go(0), v_up[0])
    when_start(v_down(0), v_dn[0])

    tail = remote(ext.at[pl.ds(ROWS, WINDOW)], ext.at[pl.ds(0, WINDOW)], ts_sem, tr_sem, sp_peer(1))
    tail.start()

    branch_start(3, 7)

    loads[L_QL].wait()
    loads[L_QC].wait()
    loads[L_QR].wait()
    lq = rms(dot(normed[...], wql[...]), qgain_ref)
    qbuf[0:128, 0:ROWS] = jnp.transpose(dot(lq, wqc[...])).astype(BF16)
    qbuf[128:192, 0:ROWS] = rotate_t(contract(wqrt[...], lq, 1, 1)).astype(BF16)
    slots = [pl.ds(d * ROWS, ROWS) for d in range(NX)]
    q_cp = [
        remote(qbuf.at[:, slots[0]], qbuf.at[:, slots[d]], qs_sem.at[d - 1], qr_sem.at[d - 1], x_peer(d))
        for d in (2, 1, 3)
    ]
    for cp in q_cp:
        cp.start()

    branch_start(4)

    loads[L_Q].wait()
    qwin[...] = dot(normed[...], wq[...]).astype(BF16)
    loads[L_GW].wait()
    loads[L_GL].wait()
    gatew[...] = jax.nn.sigmoid(dot(normed[...], wgw[...]))
    gatel[...] = jax.nn.sigmoid(dot(normed[...], wgl[...]))

    def windowed():
        tail.wait_recv()
        ki = lax.broadcasted_iota(jnp.int32, (256, 256), 0)
        ci = lax.broadcasted_iota(jnp.int32, (256, 256), 1)
        offset = jnp.where(ci < 128, ci, ci - 128) + WINDOW - ki
        band = (offset >= 0) & (offset < WINDOW)
        first = lax.broadcasted_iota(jnp.int32, (1, 256), 1) < 128
        sink = jnp.where(first, sink_ref[0], sink_ref[1])
        for n in range(ROWS // WINDOW):
            lo = n * WINDOW
            q2 = jnp.concatenate([qwin[lo : lo + 128, 0:64], qwin[lo : lo + 128, 64:128]], axis=0)
            kv = ext[lo : lo + 256, :]
            s = contract(kv[:, 0:64], q2, 1, 1) * HEAD ** (-0.5)
            valid = band & (sp * ROWS + lo - WINDOW + ki >= 0)
            s = jnp.where(valid, s, NEGATIVE)
            peak = jnp.maximum(jnp.max(s, axis=0, keepdims=True), sink)
            w = jnp.where(valid, jnp.exp(s - peak), 0.0)
            den = jnp.sum(w, axis=0, keepdims=True) + jnp.exp(sink - peak)
            p = (w / den).astype(BF16)
            o = contract(p, kv[:, 64:128], 0, 0).astype(BF16)
            wout[0, lo : lo + 128, :] = jnp.concatenate([o[:128], o[128:]], axis=1)
        direct_first(w_cp)

    w_cp = direct(wout, ws_sem, wr_sem)

    m_s[...] = jnp.full((1, NX * ROWS), NEGATIVE, F32)
    l_s[...] = jnp.zeros((1, NX * ROWS), F32)
    acc[...] = jnp.zeros((VDIM, NX * ROWS), F32)

    def tile(keys, vals, cols, masked):
        s = dot(keys, qbuf[:, cols])
        if masked:
            kpos = lax.broadcasted_iota(jnp.int32, (ROWS, ROWS), 0)
            qpos = lax.broadcasted_iota(jnp.int32, (ROWS, ROWS), 1)
            s = jnp.where(kpos <= qpos, s, NEGATIVE)
        m_old = m_s[:, cols]
        m_new = jnp.maximum(m_old, jnp.max(s, axis=0, keepdims=True))
        p = jnp.exp2((s - m_new) * SOFT)
        alpha = jnp.exp2((m_old - m_new) * SOFT)
        m_s[:, cols] = m_new
        l_s[:, cols] = l_s[:, cols] * alpha + jnp.sum(p, axis=0, keepdims=True)
        acc[:, cols] = acc[:, cols] * alpha + dot(vals, p.astype(BF16))

    def block(slot):
        keys = jnp.concatenate([kbuf[slot], jnp.transpose(rbuf[slot])], axis=1)
        return keys, vbuf[slot]

    def whole(slot):
        @pl.when(useful[slot])
        def _():
            r_hand[slot - 1][0].wait_recv()
            keys, vals = block(slot)
            tile(keys, vals, pl.ds(0, NX * ROWS), False)

    def own_square():
        keys, vals = block(0)
        tile(keys, vals, slots[0], True)

    def own_rest():
        keys, vals = block(0)
        for d in range(1, NX):

            @pl.when(d > x)
            def _():
                tile(keys, vals, slots[d], False)

    def relay(got, arrived, go, onward):
        for i, cp in enumerate(arrived):
            when_recv(got, [cp])
            if onward is not None:
                when_start(go, [onward[i]])

    def relay_k(k):
        more = k < 3
        for h in range(2):
            relay(up_got(k), k_up[k - 1][h : h + 1], up_go(k), k_up[k][h : h + 1] if more else None)
            relay(k_down(k), k_dn[k - 1][h : h + 1], k_down(k), (k_dn[k] if more else k_far)[h : h + 1])
        relay(up_got(k), r_up[k - 1], up_go(k), r_up[k] if more else None)
        when_start(useful[k], r_hand[k - 1])
        relay(k_down(k), r_dn[k - 1], k_down(k), r_dn[k] if more else r_far)
        when_start(useful[k + 3], r_hand[k + 2])

    def relay_v(k):
        for h in range(2):
            relay(up_got(k), v_up[k - 1][h : h + 1], up_go(k), v_up[k][h : h + 1])
            relay(v_down(k), v_dn[k - 1][h : h + 1], v_down(k), v_dn[k][h : h + 1])

    relay_k(1)
    own_square()
    relay_v(1)
    branch_start(5)
    relay_k(2)
    windowed()
    relay_v(2)
    for cp in q_cp:
        cp.wait_recv()
    own_rest()
    whole(1)
    relay_k(3)
    for h in range(2):
        relay((z >= 3) & (z < NZ - 1), v_up[2][h : h + 1], up_go(3), v_far[h : h + 1])
    whole(4)
    whole(2)
    when_recv(z == NZ - 1, v_up[2])
    when_recv(v_down(3), v_dn[2])
    direct_second(w_cp)
    whole(5)
    whole(3)
    whole(6)
    when_recv(z >= 4, k_far)
    when_recv(z >= 4, r_far)
    when_start(z >= 4, r_hand[6])
    when_recv(z >= 4, v_far)
    whole(7)

    pieces = [pl.ds(p * 128, 128) for p in range(3)]
    st_cp, o_cp = [], [[], [], []]
    for d in (2, 1, 3):
        st_send[d - 1, 0:1] = m_s[:, slots[d]]
        st_send[d - 1, 1:2] = l_s[:, slots[d]]
        st_cp.append(remote(st_send.at[d - 1], st_recv.at[d - 1], ss_sem.at[d - 1], sr_sem.at[d - 1], x_peer(-d)))
    for cp in st_cp:
        cp.start()
    for p in range(3):
        for d in (2, 1, 3):
            i = (d - 1) * 3 + p
            o_send[i] = acc[:, pl.ds(d * ROWS + p * 128, 128)].astype(BF16)
            o_cp[p].append(remote(o_send.at[i], o_recv.at[i], os_sem.at[i], or_sem.at[i], x_peer(-d)))
            o_cp[p][-1].start()

    blocks = [cp for slot in range(1, NTP) for cp in branch[slot]]
    for cp in blocks:
        cp.wait_recv()
    loads[L_BW].wait()
    loads[L_BL].wait()
    for cp in [w_cp[0][3]] + w_cp[1]:
        cp.wait_recv()
    allw = jnp.concatenate([wout[d] for d in range(NTP)], axis=1)
    gatew[...] = gatew[...] * dot(allw, colw[...].reshape(NTP * 128, COLS))

    l_cp = [direct(lat, ls_sem, lr_sem, p * 128, 128, p * 7) for p in range(3)]
    for cp in st_cp:
        cp.wait_recv()
    for p, cols in enumerate(pieces):
        for cp in o_cp[p]:
            cp.wait_recv()
        ms = [m_s[:, cols]] + [st_recv[d, 0:1, cols] for d in range(3)]
        ls = [l_s[:, cols]] + [st_recv[d, 1:2, cols] for d in range(3)]
        top_m = jnp.maximum(jnp.maximum(ms[0], ms[1]), jnp.maximum(ms[2], ms[3]))
        ws = [jnp.exp2((m - top_m) * SOFT) for m in ms]
        den = ls[0] * ws[0] + ls[1] * ws[1] + ls[2] * ws[2] + ls[3] * ws[3]
        o = acc[:, cols] * ws[0]
        for d in range(3):
            o = o + o_recv[d * 3 + p].astype(F32) * ws[d + 1]
        lat[0, cols] = jnp.transpose(o / den).astype(BF16)
        direct_first(l_cp[p])
    for cp in l_cp:
        direct_second(cp)
    for cp in l_cp:
        cp[0][3].wait_recv()

    def branch_part(first, count):
        rows = jnp.concatenate([lat[i] for i in range(first, first + count)], axis=1)
        return dot(rows, coll[first : first + count].reshape(count * 128, COLS))

    mixed = branch_part(0, 2)
    for cp in l_cp:
        cp[1][0].wait_recv()
        cp[1][1].wait_recv()
    mixed = mixed + branch_part(2, 2) + branch_part(6, 2)
    for cp in l_cp:
        cp[1][2].wait_recv()
    mixed = mixed + branch_part(4, 2)
    out_ref[...] = (gatew[...] + gatel[...] * mixed).astype(BF16)

    sent = list(f_cp[0].values()) + list(f_cp[1].values()) + w_cp[0] + w_cp[1] + blocks + q_cp + [tail] + st_cp
    for p in range(3):
        sent += l_cp[p][0] + l_cp[p][1] + o_cp[p]
    for k in range(3):
        when_sent(up_go(k), k_up[k])
        when_sent(up_go(k), v_up[k])
        when_sent(k_down(k), k_dn[k])
        when_sent(v_down(k), v_dn[k])
        when_sent(up_go(k), r_up[k])
        when_sent(k_down(k), r_dn[k])
    for slot in range(1, 8):
        when_sent(useful[slot], r_hand[slot - 1])
    when_sent(k_down(3), k_far)
    when_sent(k_down(3), r_far)
    when_sent(up_go(3), v_far)
    for cp in sent:
        cp.wait_send()


def on_device(
    features, norm_gain, w_query, w_key, w_value, head_sinks, w_query_latent, w_kv_latent, w_rope_key,
    query_latent_gain, kv_latent_gain, w_query_content, w_query_rotary, w_key_up, w_value_up,
    w_branch_window, w_branch_latent, w_gate_window, w_gate_latent,
):
    vmem = pl.BlockSpec(memory_space=pltpu.VMEM)
    anyspace = pl.BlockSpec(memory_space=pl.ANY)
    smem = pl.BlockSpec(memory_space=pltpu.SMEM)
    dma = pltpu.SemaphoreType.DMA
    scratch = [
        pltpu.VMEM((8, ROWS, COLS), BF16),
        pltpu.VMEM((ROWS, D), BF16),
    ]
    weights = [
        w_query, w_key.T, w_value.T, w_query_latent, w_kv_latent, w_rope_key.T, w_query_content, w_query_rotary.T,
        w_key_up, w_value_up, w_branch_window, w_branch_latent, w_gate_window, w_gate_latent,
    ]
    shapes = [
        (D, 128), (192, D), (D, LATENT), (D, LATENT), (LATENT, NOPE), (ROPE, LATENT), (LATENT, NOPE), (LATENT, VDIM),
        (D, COLS), (D, COLS),
    ]
    scratch += [pltpu.VMEM(shape, BF16) for shape in shapes] + [pltpu.VMEM((ROPE, ROWS), F32)]
    scratch += [
        pltpu.VMEM((NTP, 128, COLS), BF16),
        pltpu.VMEM((NTP, 128, COLS), BF16),
        pltpu.VMEM((8, ROWS, NOPE), BF16),
        pltpu.VMEM((8, VDIM, ROWS), BF16),
        pltpu.VMEM((8, ROPE, ROWS), BF16),
        pltpu.VMEM((NOPE + ROPE, NX * ROWS), BF16),
        pltpu.VMEM((ROWS + WINDOW, 128), BF16),
        pltpu.VMEM((ROWS, 128), BF16),
        pltpu.VMEM((ROWS, COLS), F32),
        pltpu.VMEM((ROWS, COLS), F32),
        pltpu.VMEM((1, NX * ROWS), F32),
        pltpu.VMEM((1, NX * ROWS), F32),
        pltpu.VMEM((VDIM, NX * ROWS), F32),
        pltpu.VMEM((9, VDIM, 128), BF16),
        pltpu.VMEM((NX - 1, 2, ROWS), F32),
        pltpu.VMEM((9, VDIM, 128), BF16),
        pltpu.VMEM((NX - 1, 2, ROWS), F32),
        pltpu.VMEM((NTP, ROWS, 128), BF16),
        pltpu.VMEM((NTP, ROWS, 128), BF16),
    ]
    scratch += [
        dma((15,)), dma((26,)), dma((26,))] + [dma((14,))] * 4 + [dma((7,))] * 4 + [
        dma((4,)), dma((4,)), dma(()), dma(()), dma((14,)), dma((14,)),
        dma((9,)), dma((9,)), dma((3,)), dma((3,)), dma((7,)), dma((7,)), dma((21,)), dma((21,)),
    ]
    return pl.pallas_call(
        layer,
        out_shape=pltpu.VMEM((ROWS, COLS), BF16),
        in_specs=[anyspace, vmem, vmem, vmem, smem] + [anyspace] * 14,
        out_specs=vmem,
        scratch_shapes=scratch,
        compiler_params=pltpu.CompilerParams(
            collective_id=0, has_side_effects=True, vmem_limit_bytes=60 * 1024 * 1024
        ),
    )(
        features, norm_gain.reshape(1, D), query_latent_gain.reshape(1, LATENT),
        kv_latent_gain.reshape(1, LATENT), head_sinks, *weights,
    )


def solution(mesh):
    return jax.shard_map(
        on_device,
        mesh=mesh,
        in_specs=(
            P("sp", "tp"), P(), P(None, "tp"), P(None, "tp"), P(None, "tp"), P("tp"), P(), P(), P(), P(), P(),
            P(None, "tp"), P(None, "tp"), P(None, "tp"), P(None, "tp"), P("tp", None), P("tp", None),
            P(None, "tp"), P(None, "tp"),
        ),
        out_specs=P("sp", "tp"),
        check_vma=False,
    )
```
